512 devices in a mesh: sp: 32 (over z, core), tp: 16 (over y, x).
Axes of the slice: x: 4, y: 4, z: 16, core: 2. Of those that a mesh axis runs over, the one named last changes fastest.
Arguments:
- query_pre: bfloat16 [16384, 2048], P('sp', 'tp'), may hold values from -6 to 6
- forget_pre: bfloat16 [16384, 2048], P('sp', 'tp'), may hold values from -8 to 8
- values_in: bfloat16 [16384, 2048], P('sp', 'tp'), may hold values from -16 to 16
- gate_pre: bfloat16 [16384, 2048], P('sp', 'tp'), may hold values from -6 to 6
- floor_gap: float32 [2048], P('tp'), may hold values from 0 to 1, as said below
- head_gain: float32 [128], replicated, may hold values from 0.1 to 1.9
- stream: bfloat16 [16384, 2048], P('sp', 'tp'), may hold values from -40 to 40
- out_proj: bfloat16 [2048, 2048], P(None, 'tp'), may hold values from -0.125 to 0.125
- norm_gain: float32 [2048], P('tp'), may hold values from 0.1 to 1.9
- route_ids: int32 [16384, 2], P('sp'), may hold values from 0 to 31, all different within a row; in each aligned block of 512 rows (0 to 511, 512 to 1023, ...) at most 64 rows name the same one
- route_weights: float32 [16384, 2], P('sp'), may hold values from 0.1 to 1.5
- expert_gate: bfloat16 [32, 2048, 2048], P('sp', None, 'tp'), may hold values from -0.125 to 0.125
- expert_up: bfloat16 [32, 2048, 2048], P('sp', None, 'tp'), may hold values from -0.125 to 0.125
- expert_down: bfloat16 [32, 2048, 2048], P('sp', None, 'tp'), may hold values from -0.125 to 0.125
- shared_gate: bfloat16 [2048, 2048], P(None, 'tp'), may hold values from -0.125 to 0.125
- shared_up: bfloat16 [2048, 2048], P(None, 'tp'), may hold values from -0.125 to 0.125
- shared_down: bfloat16 [2048, 2048], P(None, 'tp'), may hold values from -0.125 to 0.125
Outputs:
- layer_out: bfloat16 [16384, 2048], P('sp', 'tp')
The draws below stay inside these ranges and needn't reach their ends.
Inputs may be any that keep to these rules, and one draw needn't show every extreme that they name: `route_ids`: in each aligned block of 512 rows every expert is named by at most 64 rows, a bound that some block reaches; the 2 experts of a row differ. `floor_gap`: every entry is positive and at most 0.12.
All inputs are finite; a program needn't handle non-finite values.
Results may differ from the reference program's by a relative error of at most 0.008.
Values may be sent and summed in bfloat16 or wider, within the bound.
A program may use at most 64 MiB of HBM per device.

```python
import math
import jax
import jax.numpy as jnp
import numpy as np
from jax import lax

D = 2048
HEAD = 128
HEADS = 16
FE = 2048
FS = 2048
TOK_DEV = 512
SPAN = 64
TOP_K = 2
EXPERTS = 32
CAP = 64
TOKENS = 16384
N_SP = 32


def draw_forget_pre(key, part):
    first_key, second_key = jax.random.split(key)
    noise = jax.random.normal(first_key, (TOKENS, D), jnp.float32)
    offset = jax.random.uniform(second_key, (TOKENS // 32, D), jnp.float32, -2.0, 2.0)
    return jnp.clip(noise + jnp.repeat(offset, 32, axis=0), -8.0, 8.0).astype(jnp.bfloat16)


def draw_values_in(key, part):
    first_key, second_key = jax.random.split(key)
    noise = jax.random.normal(first_key, (TOKENS, D), jnp.float32)
    offset = 1.5 * jax.random.normal(second_key, (TOKENS // 32, D), jnp.float32)
    return jnp.clip(noise + jnp.repeat(offset, 32, axis=0), -16.0, 16.0).astype(jnp.bfloat16)


def draw_floor_gap(key, part):
    picker, slow_key, fast_key = jax.random.split(key, 3)
    chance = jax.random.uniform(picker, (D,), jnp.float32)
    lasting = chance < 0.5
    slow_gap = jnp.exp(jax.random.uniform(slow_key, (D,), jnp.float32, math.log(0.5), math.log(2.5))) / TOKENS
    fast_gap = jnp.exp(jax.random.uniform(fast_key, (D,), jnp.float32, math.log(0.03), math.log(0.12)))
    return jnp.where(lasting, slow_gap, fast_gap).astype(jnp.float32)


def draw_stream(key, part):
    noise_key, scale_key, row_key = jax.random.split(key, 3)
    noise = jax.random.normal(noise_key, (TOKENS, D), jnp.float32)
    scales = jnp.repeat(jnp.exp(jax.random.uniform(scale_key, (16,), jnp.float32, -1.2, 1.2)), D // 16)
    return jnp.clip(noise * scales, -40.0, 40.0).astype(jnp.bfloat16)


def shard_levels(stream_key, shape, shards, least, top_value):
    def one(position, blocks):
        draws = jax.random.uniform(jax.random.fold_in(jax.random.fold_in(stream_key, 6), position), (blocks,), jnp.float32, least / len(shards), top_value / len(shards))
        return jnp.repeat(jnp.exp(draws), shape[position] // blocks).reshape((-1,) + (1,) * (len(shape) - position - 1))

    factor_of = one(*shards[0])
    for cut in shards[1:]:
        factor_of = factor_of * one(*cut)
    return factor_of


def assign_block(stream_key, own, number, rows, number_of, top, limit, skew):
    sequence = jax.random.permutation(stream_key, number_of)
    packed, usual = load_shares(number_of, rows * top, limit, skew, True), load_shares(number_of, rows * top, limit, skew, False)
    places = jnp.arange(number_of)

    def named(lengths, rotation):
        used = int((lengths > 0).sum())
        fixed = max(1, used // 4)
        shifted = fixed + (places - fixed + rotation * (used - fixed)) % max(1, number_of - fixed)
        return jnp.zeros((number_of,), jnp.int32).at[sequence[jnp.where(places < fixed, places, shifted)]].set(jnp.asarray(lengths, jnp.int32))

    lengths = jnp.where(number % 4 == 0, named(packed, number // 4), named(usual, number - number // 4 - 1))
    mixed = jax.random.permutation(jax.random.fold_in(own, 3), number_of)
    giver, taker = mixed[0:number_of // 2 * 2:2], mixed[1:number_of // 2 * 2:2]
    margin = jnp.minimum(lengths[giver] - 1, limit - lengths[taker]) // 2
    margin = jnp.where((giver == sequence[0]) | (taker == sequence[0]) | (lengths[taker] == 0), 0, jnp.maximum(margin, 0))
    shifted = jax.random.randint(jax.random.fold_in(own, 4), (number_of // 2,), 0, 1 << 20) % (margin + 1)
    lengths = lengths.at[giver].add(-shifted).at[taker].add(shifted)
    members = jnp.searchsorted(jnp.cumsum(lengths), jnp.arange(rows * top), side="right").astype(jnp.int32)
    table = members.reshape(top, rows).T
    table = table[jax.random.permutation(jax.random.fold_in(own, 1), rows)]
    rotation = jax.random.randint(jax.random.fold_in(own, 2), (rows, 1), 0, top)
    return jnp.take_along_axis(table, (jnp.arange(top)[None, :] + rotation) % top, axis=1)


def load_shares(count, total, limit, slope, full):
    weights = [(1 << 20) // math.isqrt(grade ** slope) + 1 for grade in range(1, count + 1)]
    largest = limit if full else min(limit, max(-(-total // count), total * weights[0] // sum(weights)))
    least = 1 if total - largest >= count - 1 else 0
    counts, spare = [largest] + [least] * (count - 1), total - largest - least * (count - 1)
    while spare > 0:
        free = [i for i in range(1, count) if counts[i] < largest] or [i for i in range(1, count) if counts[i] < limit]
        mass, budget = sum([weights[i] for i in free]), spare
        for i in free:
            more = min(limit - counts[i], max(1, budget * weights[i] // mass), spare)
            counts[i] = counts[i] + more
            spare = spare - more
    return np.array(counts)


def bell_draw(key, dims, deviation, most, cuts=(), kind=jnp.bfloat16):
    factor_of = shard_levels(key, dims, cuts, -0.22, 0.18) if cuts else 1.0
    values = jax.random.normal(key, dims, jnp.float32) * deviation * factor_of
    return jnp.minimum(jnp.maximum(values, -most), most).astype(kind)


def setup_inputs(seed: int = 0) -> dict:
    arg_keys = jax.random.split(jax.random.key(seed), 18)
    query_pre = bell_draw(arg_keys[0], (TOKENS, D), 1.0, 6.0, ((0, 32), (1, 16)))
    forget_pre = draw_forget_pre(jax.random.fold_in(arg_keys[17], 71), 0)
    values_in = draw_values_in(jax.random.fold_in(arg_keys[17], 71), 0)
    gate_pre = bell_draw(arg_keys[3], (TOKENS, D), 1.0, 6.0, ((0, 32), (1, 16)))
    floor_gap = draw_floor_gap(jax.random.fold_in(arg_keys[17], 71), 0)
    head_gain = jnp.clip(1.0 + 0.18 * jax.random.normal(arg_keys[5], (HEAD,), jnp.float32), 0.1, 1.9)
    stream = draw_stream(jax.random.fold_in(arg_keys[17], 71), 0)
    out_proj = bell_draw(arg_keys[7], (D, D), D ** -0.5, 0.125, ((1, 16),))
    norm_gain = jnp.clip(1.0 + 0.18 * jax.random.normal(arg_keys[8], (D,), jnp.float32), 0.1, 1.9)
    route_ids_keys = jax.random.split(jax.random.fold_in(arg_keys[9], 1), TOKENS // TOK_DEV)
    route_ids_turns = jax.random.permutation(jax.random.fold_in(arg_keys[9], 3), TOKENS // TOK_DEV)
    route_ids = jax.vmap(lambda own, number: assign_block(jax.random.fold_in(arg_keys[9], 2), own, number, TOK_DEV, EXPERTS, TOP_K, CAP, 2))(route_ids_keys, route_ids_turns).reshape((TOKENS, TOP_K))
    route_weights = jnp.clip(0.1 + 1.4 * jax.random.uniform(arg_keys[10], (TOKENS, TOP_K), jnp.float32) ** shard_levels(arg_keys[10], (TOKENS, TOP_K), ((0, 32),), -0.2, 0.2), 0.1, 1.5)
    expert_gate = bell_draw(arg_keys[11], (EXPERTS, D, FE), D ** -0.5, 0.125, ((0, 32), (2, 16)))
    expert_up = bell_draw(arg_keys[12], (EXPERTS, D, FE), D ** -0.5, 0.125, ((0, 32), (2, 16)))
    expert_down = bell_draw(arg_keys[13], (EXPERTS, FE, D), FE ** -0.5, 0.125, ((0, 32), (2, 16)))
    shared_gate = bell_draw(arg_keys[14], (D, FS), D ** -0.5, 0.125, ((1, 16),))
    shared_up = bell_draw(arg_keys[15], (D, FS), D ** -0.5, 0.125, ((1, 16),))
    shared_down = bell_draw(arg_keys[16], (FS, D), FS ** -0.5, 0.125, ((1, 16),))
    return {"query_pre": query_pre, "forget_pre": forget_pre, "values_in": values_in, "gate_pre": gate_pre, "floor_gap": floor_gap, "head_gain": head_gain, "stream": stream, "out_proj": out_proj, "norm_gain": norm_gain, "route_ids": route_ids, "route_weights": route_weights, "expert_gate": expert_gate, "expert_up": expert_up, "expert_down": expert_down, "shared_gate": shared_gate, "shared_up": shared_up, "shared_down": shared_down}


EPS = 1e-06
HIGH = lax.Precision.HIGHEST

def span_step(memory, blocks):
    queries, leakage, values, log_keep = blocks
    length = queries.shape[1]
    growth = jnp.cumsum(log_keep, axis=1)
    causal = jnp.tril(jnp.ones((length, length), dtype=bool))
    spread = growth[:, :, None, :] - growth[:, None, :, :]
    decays = jnp.exp(jnp.where(causal[None, :, :, None], spread, -jnp.inf))
    scores = jnp.einsum('htd,hsd,htsd->hts', queries, leakage, decays, precision=HIGH)
    within = jnp.einsum('hts,hsv->htv', scores, values, precision=HIGH)
    carried = jnp.einsum('htd,hdv->htv', queries * jnp.exp(growth), memory, precision=HIGH)
    closing = growth[:, -1:, :]
    memory = jnp.exp(closing[:, 0, :, None]) * memory + jnp.einsum('hsd,hsv->hdv', leakage * jnp.exp(closing - growth), values, precision=HIGH)
    return (memory, within + carried)

def recurrence(queries, leakage, values, log_keep, memory):
    head_count, length, channels = queries.shape
    number = length // SPAN

    def blocked(array):
        return array.reshape(head_count, number, SPAN, channels).transpose(1, 0, 2, 3)
    memory, outputs = lax.scan(span_step, memory, (blocked(queries), blocked(leakage), blocked(values), blocked(log_keep)))
    return outputs.transpose(1, 0, 2, 3).reshape(head_count, length, channels)

def split_heads(array):
    return array.astype(jnp.float32).reshape(TOKENS, HEADS, HEAD).transpose(1, 0, 2)

def reference(query_pre, forget_pre, values_in, gate_pre, floor_gap, head_gain, stream, out_proj, norm_gain, route_ids, route_weights, expert_gate, expert_up, expert_down, shared_gate, shared_up, shared_down):
    queries = jax.nn.silu(split_heads(query_pre))
    leakage = floor_gap.reshape(HEADS, 1, HEAD) * jax.nn.sigmoid(-split_heads(forget_pre))
    log_keep = jnp.log1p(-leakage)
    memory = jnp.zeros((HEADS, HEAD, HEAD), jnp.float32)
    outputs = recurrence(queries, leakage, split_heads(values_in), log_keep, memory)
    scaled = outputs * lax.rsqrt(lax.optimization_barrier(jnp.mean(outputs * outputs, axis=2, keepdims=True)) + EPS) * head_gain
    gated = scaled * jax.nn.silu(split_heads(gate_pre))
    mixed = gated.transpose(1, 0, 2).reshape(TOKENS, D).astype(jnp.bfloat16)
    residual = stream.astype(jnp.float32) + jnp.dot(mixed, out_proj, preferred_element_type=jnp.float32)
    normed = (residual * lax.rsqrt(lax.optimization_barrier(jnp.mean(residual * residual, axis=1, keepdims=True)) + EPS) * norm_gain).astype(jnp.bfloat16)
    shared_hidden = (jax.nn.silu(jnp.dot(normed, shared_gate, preferred_element_type=jnp.float32)) * jnp.dot(normed, shared_up, preferred_element_type=jnp.float32)).astype(jnp.bfloat16)
    shared_out = jnp.dot(shared_hidden, shared_down, preferred_element_type=jnp.float32)
    flat_ids = route_ids.reshape(-1)
    flat_weights = route_weights.reshape(-1)
    most_rows = N_SP * CAP

    def one_expert(routed, expert):
        hitting = flat_ids == expert
        chosen = jnp.nonzero(hitting, size=most_rows, fill_value=0)[0].astype(jnp.int32)
        filled = jnp.arange(most_rows, dtype=jnp.int32) < jnp.sum(hitting.astype(jnp.int32))
        tokens = (chosen // TOP_K).astype(jnp.int32)
        gathered = normed[tokens]
        hidden = (jax.nn.silu(jnp.dot(gathered, expert_gate[expert], preferred_element_type=jnp.float32)) * jnp.dot(gathered, expert_up[expert], preferred_element_type=jnp.float32)).astype(jnp.bfloat16)
        result = jnp.dot(hidden, expert_down[expert], preferred_element_type=jnp.float32).astype(jnp.bfloat16)
        result = lax.optimization_barrier(result).astype(jnp.float32)
        weights = jnp.where(filled, flat_weights[chosen], 0.0)
        return (routed.at[tokens].add(result * weights[:, None]), None)
    routed, unused = lax.scan(one_expert, jnp.zeros((TOKENS, D), jnp.float32), jnp.arange(EXPERTS, dtype=jnp.int32))
    return (residual + shared_out + routed).astype(jnp.bfloat16)
```

```python
import functools

import jax
import jax.numpy as jnp
from jax import lax
from jax.experimental import pallas as pl
from jax.experimental.pallas import tpu as pltpu
from jax.sharding import Mesh
from jax.sharding import PartitionSpec as P

D = 2048
T = 512
W = 128
CAP = 64
EPS = 1e-06
MESH = pl.DeviceIdType.MESH
F32 = jnp.float32
BF16 = jnp.bfloat16


class Sems:
    def __init__(self):
        self.used = 0

    def take(self, count):
        first = self.used
        self.used += count
        return first


SEM = Sems()
LOCAL_W = SEM.take(7)
GATHER_W = [(SEM.take(3), SEM.take(3)) for _ in range(3)]
PAIR = SEM.take(2)
PAIR_H = SEM.take(2)
STATE_S, STATE_R = SEM.take(16), SEM.take(16)
DECAY_S, DECAY_R = SEM.take(16), SEM.take(16)
SQUARE_S, SQUARE_R = SEM.take(16), SEM.take(16)
OUT_S, OUT_R = SEM.take(32), SEM.take(32)
BACK_S, BACK_R = SEM.take(32), SEM.take(32)
ALONG_A = [(SEM.take(3), SEM.take(3)) for _ in range(5)]
ALONG_B = [[SEM.take(4) for _ in range(8)] for _ in range(5)]


def dot(left, right):
    return jnp.dot(left, right, preferred_element_type=F32)


def dot_last(left, right):
    return lax.dot_general(left, right, (((1,), (1,)), ((), ())), preferred_element_type=F32)


def dot_first(left, right):
    return lax.dot_general(left, right, (((0,), (0,)), ((), ())), preferred_element_type=F32)


def silu(v):
    return v * jax.nn.sigmoid(v)


def in_three(value):
    high = value.astype(BF16)
    rest = value - high.astype(F32)
    middle = rest.astype(BF16)
    low = (rest - middle.astype(F32)).astype(BF16)
    return high, middle, low


def diagonal():
    return lax.broadcasted_iota(jnp.int32, (W, W), 0) == lax.broadcasted_iota(jnp.int32, (W, W), 1)


def to_column(row):
    eye = diagonal()
    return jnp.concatenate(
        [
            jnp.sum(jnp.where(eye, row[:, k * W : (k + 1) * W], 0.0), axis=1, keepdims=True)
            for k in range(row.shape[1] // W)
        ],
        axis=0,
    )


def to_row(column):
    eye = diagonal()
    return jnp.concatenate(
        [
            jnp.sum(jnp.where(eye, column[k * W : (k + 1) * W], 0.0), axis=0, keepdims=True)
            for k in range(column.shape[0] // W)
        ],
        axis=1,
    )


def kernel(
    zs,
    query_ref,
    forget_ref,
    value_ref,
    gatep_ref,
    gap_ref,
    head_gain_ref,
    stream_ref,
    norm_gain_ref,
    ids_ref,
    weights_ref,
    proj_hbm,
    sg_hbm,
    su_hbm,
    sd_hbm,
    eg_hbm,
    eu_hbm,
    ed_hbm,
    out_ref,
    wo,
    wsg,
    wsu,
    wsd,
    weg,
    weu,
    wed,
    pair_mine,
    pair_other,
    state_send,
    state_recv,
    decay_send,
    decay_recv,
    half_mine,
    half_other,
    squares,
    x_mixed,
    x_normed,
    x_shared,
    x_rows,
    x_hidden,
    send_rows,
    recv_rows,
    result,
    gathered,
    back,
    choose,
    pick0,
    pick1,
    residual,
    shared_out,
    within,
    carried,
    gate_act,
    slots,
    sems,
):
    z, c = lax.axis_index("z"), lax.axis_index("c")
    y, x = lax.axis_index("y"), lax.axis_index("x")
    me = z * 2 + c
    spn = zs * 2
    j = y * 4 + x
    a = x * (1 - c) + y * c
    b = y * (1 - c) + x * c
    group = spn * CAP // 4

    def plane(a_to, b_to):
        return (z, c, b_to * (1 - c) + a_to * c, a_to * (1 - c) + b_to * c)

    def number(a_to, b_to):
        return (b_to * (1 - c) + a_to * c) * 4 + a_to * (1 - c) + b_to * c

    def column(number_of):
        return pl.ds(pl.multiple_of(number_of * W, W), W)

    def rows_of(number_of, count):
        return pl.ds(pl.multiple_of(number_of * count, count), count)

    def remote(src, dst, sent, received, where):
        return pltpu.make_async_remote_copy(
            src_ref=src,
            dst_ref=dst,
            send_sem=sems.at[sent],
            recv_sem=sems.at[received],
            device_id=where,
            device_id_type=MESH,
        )

    barrier = pltpu.get_barrier_semaphore()

    def greet_column(i, carry):
        to = (me + i) % spn
        pl.semaphore_signal(barrier, inc=1, device_id=(to // 2, to % 2, y, x), device_id_type=MESH)
        return carry

    def greet_plane(i, carry):
        to = (j + i) % 16
        pl.semaphore_signal(barrier, inc=1, device_id=(z, c, to // 4, to % 4), device_id_type=MESH)
        return carry

    lax.fori_loop(1, spn, greet_column, 0)
    lax.fori_loop(1, 16, greet_plane, 0)

    local = [
        pltpu.make_async_copy(src, dst, sems.at[LOCAL_W + k])
        for k, (src, dst) in enumerate(
            [
                (eg_hbm, weg.at[:, column(a)]),
                (proj_hbm, wo),
                (sg_hbm, wsg),
                (su_hbm, wsu),
                (sd_hbm, wsd),
                (eu_hbm, weu.at[:, column(a)]),
                (ed_hbm, wed.at[:, column(a)]),
            ]
        )
    ]
    for copy in local:
        copy.start()

    leakage = gap_ref[...] * jax.nn.sigmoid(-forget_ref[...].astype(F32))
    log_keep = jnp.log1p(-leakage)
    lower = (
        lax.broadcasted_iota(jnp.int32, (T, T), 0) >= lax.broadcasted_iota(jnp.int32, (T, T), 1)
    ).astype(BF16)
    high, middle, low = in_three(log_keep)
    growth = dot(lower, high) + dot(lower, middle) + dot(lower, low)
    closing = growth[T - 1 : T, :]
    values = value_ref[...]
    state = dot_first(values, (leakage * jnp.exp(closing - growth)).astype(BF16))
    through = jnp.exp(closing)
    pair_mine[0:W, :] = state
    pair_mine[W : W + 8, :] = jnp.broadcast_to(through, (8, W))

    pl.semaphore_wait(barrier, spn - 1 + 15)

    swap = remote(pair_mine, pair_other, PAIR, PAIR + 1, (z, 1 - c, y, x))
    swap.start()

    def gather_weights(which, src, dst):
        sent, received = GATHER_W[which]
        copies = []
        for i in (1, 3, 2):
            copies.append(
                remote(src, dst.at[:, column(a)], sent + i - 1, received + i - 1, plane((a + i) % 4, b))
            )
        for copy in copies:
            copy.start()

        def finish():
            local[{0: 0, 1: 5, 2: 6}[which]].wait()
            for i in (1, 3, 2):
                from_a = (a + 4 - i) % 4
                remote(
                    src, dst.at[:, column(from_a)], sent + i - 1, received + i - 1, plane(from_a, b)
                ).wait_recv()

        return copies, finish

    gate_copies, gate_ready = gather_weights(0, eg_hbm, weg)

    swap.wait_recv()
    other_state, other_through = pair_other[0:W, :], pair_other[W : W + 1, :]
    mine_first = c == 0
    first = jnp.where(mine_first, state, other_state)
    second = jnp.where(mine_first, other_state, state)
    second_through = jnp.where(mine_first, other_through, through)
    total = first * second_through + second
    state_send[...] = jnp.where(mine_first, total[0:CAP, :], total[CAP:W, :]).astype(BF16)
    decay_send[...] = through * other_through

    def state_copy(to, slot):
        return remote(state_send, state_recv.at[slot], STATE_S + to, STATE_R + slot, (to, c, y, x))

    def decay_copy(to, slot):
        return remote(decay_send, decay_recv.at[slot], DECAY_S + to, DECAY_R + slot, (to, c, y, x))

    def send_state(i, carry):
        to = zs - 1 - i
        state_copy(to, z).start()
        decay_copy(to, z).start()
        return carry

    lax.fori_loop(0, zs - 1 - z, send_state, 0)

    queries = silu(query_ref[...].astype(F32))
    centre = growth[T // 2 - 1 : T // 2, :]
    scaled_q = (queries * jnp.exp(growth - centre)).astype(BF16)
    scaled_k = (leakage * jnp.exp(centre - growth)).astype(BF16)
    carried[...] = (queries * jnp.exp(growth)).astype(BF16)
    gate_act[...] = silu(gatep_ref[...].astype(F32)) * head_gain_ref[...]
    for k in range(T // W):
        upto = (k + 1) * W
        scores = dot_last(scaled_q[k * W : upto, :], scaled_k[0:upto, :])
        causal = lax.broadcasted_iota(jnp.int32, (W, upto), 0) + k * W >= lax.broadcasted_iota(
            jnp.int32, (W, upto), 1
        )
        scores = jnp.where(causal, scores, 0.0).astype(BF16)
        within[k * W : upto, :] = dot(scores, values[0:upto, :])

    ids = ids_ref[...]
    lanes = lax.broadcasted_iota(jnp.int32, (W, T), 0)
    hits0, hits1 = lanes == ids[0:1, :], lanes == ids[1:2, :]
    before = (
        lax.broadcasted_iota(jnp.int32, (T, T), 0) < lax.broadcasted_iota(jnp.int32, (T, T), 1)
    ).astype(BF16)
    earlier = dot((hits0 | hits1).astype(BF16), before)
    place = earlier + lanes.astype(F32) * CAP
    slot0 = jnp.sum(jnp.where(hits0, place, 0.0), axis=0, keepdims=True)
    slot1 = jnp.sum(jnp.where(hits1, place, 0.0), axis=0, keepdims=True)
    slots[0] = jnp.broadcast_to(to_column(slot0), (T, W))
    slots[1] = jnp.broadcast_to(to_column(slot1), (T, W))

    def build(i, carry):
        base = (i * W).astype(F32)
        down = lax.broadcasted_iota(jnp.int32, (W, T), 0).astype(F32) + base
        choose[rows_of(i, W), :] = ((down == slot0) | (down == slot1)).astype(BF16)
        along = lax.broadcasted_iota(jnp.int32, (T, W), 1).astype(F32) + base
        pick0[:, column(i)] = (slots[0] == along).astype(BF16)
        pick1[:, column(i)] = (slots[1] == along).astype(BF16)
        return carry

    lax.fori_loop(0, spn * CAP // W, build, 0)

    def take_state(k, held):
        state_copy(k, k).wait_recv()
        decay_copy(k, k).wait_recv()
        return held * decay_recv[k] + state_recv[k].astype(F32)

    half = lax.fori_loop(0, z, take_state, jnp.zeros((CAP, W), F32))
    half_mine[...] = half
    swap_half = remote(half_mine, half_other, PAIR_H, PAIR_H + 1, (z, 1 - c, y, x))
    swap_half.start()
    swap_half.wait_recv()
    theirs = half_other[...]
    incoming = jnp.concatenate(
        [jnp.where(mine_first, half, theirs), jnp.where(mine_first, theirs, half)], axis=0
    )
    incoming = jnp.where(
        mine_first, incoming, incoming * pair_other[W : W + 1, :] + pair_other[0:W, :]
    )
    outputs = within[...] + dot_last(carried[...], incoming.astype(BF16))
    mean = jnp.mean(outputs * outputs, axis=1, keepdims=True)
    x_mixed[:, column(j)] = (outputs * lax.rsqrt(mean + EPS) * gate_act[...]).astype(BF16)

    def gather_along_b(buffer, which, order, ready):
        sems_of = ALONG_B[which]
        rows = buffer.shape[0]
        upper, lower_half = pl.ds(0, rows // 2), pl.ds(rows // 2, rows // 2)
        every = pl.ds(0, rows)
        right, left = (b + 1) % 4, (b + 3) % 4
        sends = []

        def step(i, part, b_of, to, kind):
            block = buffer.at[part, column(number((a + 4 - i) % 4, b_of))]
            return remote(block, block, sems_of[2 * kind] + i, sems_of[2 * kind + 1] + i, plane(a, to))

        def start(copy):
            copy.start()
            sends.append(copy)

        def forward(i):
            step(i, every, left, right, 0).wait_recv()
            start(step(i, upper, left, right, 2))
            step(i, every, right, left, 1).wait_recv()
            start(step(i, lower_half, right, left, 3))

        last = None
        for i in order:
            ready(i)
            start(step(i, every, b, right, 0))
            start(step(i, every, b, left, 1))
            if last is not None:
                forward(last)
            last = i
        forward(last)

        def finish():
            opposite = (b + 2) % 4
            for i in order:
                step(i, upper, opposite, right, 2).wait_recv()
                step(i, lower_half, opposite, left, 3).wait_recv()
            return sends

        return finish

    def send_along_a(which, source_of, buffer):
        sent, received = ALONG_A[which]
        copies = []
        for i in (1, 3, 2):
            to = (a + i) % 4
            copies.append(
                remote(source_of(to), buffer.at[:, column(j)], sent + i - 1, received + i - 1, plane(to, b))
            )
            copies[-1].start()

        def ready(i):
            if i:
                from_a = (a + 4 - i) % 4
                block = buffer.at[:, column(number(from_a, b))]
                remote(block, block, sent + i - 1, received + i - 1, plane(from_a, b)).wait_recv()

        return copies, ready

    def gather_plane(buffer, which):
        own = buffer.at[:, column(j)]
        copies, ready = send_along_a(which, lambda to: own, buffer)
        finish = gather_along_b(buffer, which, (0, 1, 3, 2), ready)
        return lambda: copies + finish()

    pending = list(gate_copies)
    finish = gather_plane(x_mixed, 0)
    pending += finish()
    up_copies, up_ready = gather_weights(1, eu_hbm, weu)
    pending += up_copies

    local[1].wait()
    res = stream_ref[...].astype(F32) + dot(x_mixed[...], wo[...])
    residual[...] = res
    squares[j] = to_row(jnp.sum(res * res, axis=1, keepdims=True))

    def square_copy(to, slot):
        return remote(
            squares.at[slot], squares.at[slot], SQUARE_S + to, SQUARE_R + slot, (z, c, to // 4, to % 4)
        )

    def send_squares(i, carry):
        square_copy((j + i) % 16, j).start()
        return carry

    def wait_squares(i, carry):
        square_copy((j + i) % 16, (j + i) % 16).wait_recv()
        return carry

    lax.fori_loop(1, 16, send_squares, 0)
    lax.fori_loop(1, 16, wait_squares, 0)
    summed = jnp.sum(squares[...], axis=0)
    scale = to_column(lax.rsqrt(summed / D + EPS))
    normed = (res * scale * norm_gain_ref[...]).astype(BF16)
    x_normed[:, column(j)] = normed

    for k in range(spn * CAP // T):
        send_rows[k * T : (k + 1) * T, :] = dot(choose[k * T : (k + 1) * T, :], normed).astype(BF16)

    def out_copy(to, slot):
        return remote(
            send_rows.at[rows_of(to, CAP), :],
            recv_rows.at[rows_of(slot, CAP), :],
            OUT_S + to,
            OUT_R + slot,
            (to // 2, to % 2, y, x),
        )

    def send_out(i, carry):
        out_copy((me + i) % spn, me).start()
        return carry

    def wait_out(i, carry):
        out_copy((me + i) % spn, (me + i) % spn).wait_recv()
        return carry

    lax.fori_loop(1, spn, send_out, 0)
    recv_rows[rows_of(me, CAP), :] = send_rows[rows_of(me, CAP), :]

    finish = gather_plane(x_normed, 1)
    pending += finish()
    local[2].wait()
    local[3].wait()
    hidden = silu(dot(x_normed[...], wsg[...])) * dot(x_normed[...], wsu[...])
    x_shared[:, column(j)] = hidden.astype(BF16)
    finish = gather_plane(x_shared, 2)
    down_copies, down_ready = gather_weights(2, ed_hbm, wed)
    pending += down_copies
    pending += finish()
    local[4].wait()
    shared_out[...] = residual[...] + dot(x_shared[...], wsd[...])

    lax.fori_loop(1, spn, wait_out, 0)
    own_rows = pl.ds(pl.multiple_of(a * group, group), group)
    x_rows[:, column(j)] = recv_rows[own_rows, :]
    copies, ready = send_along_a(3, lambda to: recv_rows.at[rows_of(to, group), :], x_rows)
    pending += copies
    pending += gather_along_b(x_rows, 3, (0, 1, 3, 2), ready)()
    gate_ready()
    up_ready()
    for k in range(4):
        part = slice(k * (group // 4), (k + 1) * (group // 4))
        rows_in = x_rows[part, :]
        hidden = (silu(dot(rows_in, weg[...])) * dot(rows_in, weu[...])).astype(BF16)
        for n in range(4):
            x_hidden[part, column(number(n, b))] = hidden[:, n * W : (n + 1) * W]
    pending += gather_along_b(x_hidden, 4, (0, 1, 2, 3), lambda i: None)()
    down_ready()
    for k in range(4):
        part = slice(k * (group // 4), (k + 1) * (group // 4))
        rows_out = dot(x_hidden[part, :], wed[...]).astype(BF16)
        for n in range(4):
            result[n, part, :] = rows_out[:, n * W : (n + 1) * W]

    sent, received = ALONG_A[4]
    for i in (1, 3, 2):
        to = (a + i) % 4
        copy = remote(
            result.at[to], gathered.at[own_rows, :], sent + i - 1, received + i - 1, plane(to, b)
        )
        copy.start()
        pending.append(copy)
    gathered[own_rows, :] = result[a]
    for i in (1, 3, 2):
        from_a = (a + 4 - i) % 4
        remote(
            result.at[a], gathered.at[rows_of(from_a, group), :], sent + i - 1, received + i - 1, plane(from_a, b)
        ).wait_recv()

    def back_copy(to, slot):
        return remote(
            gathered.at[rows_of(to, CAP), :],
            back.at[rows_of(slot, CAP), :],
            BACK_S + to,
            BACK_R + slot,
            (to // 2, to % 2, y, x),
        )

    def send_back(i, carry):
        back_copy((me + i) % spn, me).start()
        return carry

    def wait_back(i, carry):
        back_copy((me + i) % spn, (me + i) % spn).wait_recv()
        return carry

    lax.fori_loop(1, spn, send_back, 0)
    back[rows_of(me, CAP), :] = gathered[rows_of(me, CAP), :]
    lax.fori_loop(1, spn, wait_back, 0)

    returned = back[...]
    weights = weights_ref[...]
    routed = dot(pick0[...], returned) * to_column(weights[0:1, :])
    routed += dot(pick1[...], returned) * to_column(weights[1:2, :])
    out_ref[...] = (shared_out[...] + routed).astype(BF16)

    swap.wait_send()
    swap_half.wait_send()
    for copy in pending:
        copy.wait_send()

    def drain_state(i, carry):
        state_copy(zs - 1 - i, z).wait_send()
        decay_copy(zs - 1 - i, z).wait_send()
        return carry

    def drain_squares(i, carry):
        square_copy((j + i) % 16, j).wait_send()
        return carry

    def drain_rows(i, carry):
        out_copy((me + i) % spn, me).wait_send()
        back_copy((me + i) % spn, me).wait_send()
        return carry

    lax.fori_loop(0, zs - 1 - z, drain_state, 0)
    lax.fori_loop(1, 16, drain_squares, 0)
    lax.fori_loop(1, spn, drain_rows, 0)


def layer(zs, *args):
    (
        query_pre,
        forget_pre,
        values_in,
        gate_pre,
        floor_gap,
        head_gain,
        stream,
        out_proj,
        norm_gain,
        route_ids,
        route_weights,
        expert_gate,
        expert_up,
        expert_down,
        shared_gate,
        shared_up,
        shared_down,
    ) = args
    rows = zs * 2 * CAP
    group = rows // 4
    vmem = pl.BlockSpec(memory_space=pltpu.VMEM)
    hbm = pl.BlockSpec(memory_space=pl.ANY)
    scratch = [
        *[pltpu.VMEM((D, W), BF16)] * 4,
        *[pltpu.VMEM((D, 4 * W), BF16)] * 3,
        *[pltpu.VMEM((W + 8, W), F32)] * 2,
        pltpu.VMEM((CAP, W), BF16),
        pltpu.VMEM((zs, CAP, W), BF16),
        pltpu.VMEM((1, W), F32),
        pltpu.VMEM((zs, 1, W), F32),
        *[pltpu.VMEM((CAP, W), F32)] * 2,
        pltpu.VMEM((16, 1, T), F32),
        *[pltpu.VMEM((T, D), BF16)] * 3,
        *[pltpu.VMEM((group, D), BF16)] * 2,
        *[pltpu.VMEM((rows, W), BF16)] * 2,
        pltpu.VMEM((4, group, W), BF16),
        *[pltpu.VMEM((rows, W), BF16)] * 2,
        pltpu.VMEM((rows, T), BF16),
        *[pltpu.VMEM((T, rows), BF16)] * 2,
        *[pltpu.VMEM((T, W), F32)] * 3,
        pltpu.VMEM((T, W), BF16),
        pltpu.VMEM((T, W), F32),
        pltpu.VMEM((2, T, W), F32),
        pltpu.SemaphoreType.DMA((SEM.used,)),
    ]
    return pl.pallas_call(
        functools.partial(kernel, zs),
        out_shape=jax.ShapeDtypeStruct((T, W), BF16),
        in_specs=[vmem] * 10 + [hbm] * 7,
        out_specs=vmem,
        scratch_shapes=scratch,
        compiler_params=pltpu.CompilerParams(
            collective_id=0, has_side_effects=True, vmem_limit_bytes=60 * 1024 * 1024
        ),
        name="layer",
    )(
        query_pre,
        forget_pre,
        values_in,
        gate_pre,
        floor_gap.reshape(1, W),
        head_gain.reshape(1, W),
        stream,
        norm_gain.reshape(1, W),
        route_ids.T,
        route_weights.T,
        out_proj,
        shared_gate,
        shared_up,
        shared_down,
        expert_gate.reshape(D, W),
        expert_up.reshape(D, W),
        expert_down.reshape(D, W),
    )


def solution(mesh):
    zs = mesh.shape["sp"] // 2
    finer = Mesh(mesh.devices.reshape(zs, 2, 4, 4), ("z", "c", "y", "x"))
    sp, tp = ("z", "c"), ("y", "x")
    in_specs = (
        P(sp, tp),
        P(sp, tp),
        P(sp, tp),
        P(sp, tp),
        P(tp),
        P(),
        P(sp, tp),
        P(None, tp),
        P(tp),
        P(sp, None),
        P(sp, None),
        P(sp, None, tp),
        P(sp, None, tp),
        P(sp, None, tp),
        P(None, tp),
        P(None, tp),
        P(None, tp),
    )
    return jax.shard_map(
        functools.partial(layer, zs),
        mesh=finer,
        in_specs=in_specs,
        out_specs=P(sp, tp),
        check_vma=False,
    )
```

```python
import functools

import jax
import jax.numpy as jnp
from jax import lax
from jax.experimental import pallas as pl
from jax.experimental.pallas import tpu as pltpu
from jax.sharding import Mesh
from jax.sharding import PartitionSpec as P

D = 2048
T = 512
W = 128
CAP = 64
EPS = 1e-06
MESH = pl.DeviceIdType.MESH
F32 = jnp.float32
BF16 = jnp.bfloat16


class Sems:
    def __init__(self):
        self.used = 0

    def take(self, count):
        first = self.used
        self.used += count
        return first


SEM = Sems()
CHUNKS = 2
CH = CAP // CHUNKS
INPUTS = SEM.take(17)
OUTPUT = SEM.take(1)
WEIGHTS = [SEM.take(5) for _ in range(3)]
PAIR = SEM.take(2)
PAIR_H = SEM.take(2)
NEAR_S, NEAR_R = SEM.take(8), SEM.take(8)
STATE_S, STATE_R = SEM.take(16), SEM.take(4)
DECAY_S, DECAY_R = SEM.take(16), SEM.take(4)
SQUARE = SEM.take(2)
OUT = [SEM.take(2) for _ in range(CHUNKS)]
BACK = [SEM.take(2) for _ in range(CHUNKS)]
ALONG_A = [SEM.take(4) for _ in range(3 + 2 * CHUNKS)]
ALONG_B = [SEM.take(17) for _ in range(3 + 2 * CHUNKS)]


def dot(left, right):
    return jnp.dot(left, right, preferred_element_type=F32)


def dot_last(left, right):
    return lax.dot_general(left, right, (((1,), (1,)), ((), ())), preferred_element_type=F32)


def dot_first(left, right):
    return lax.dot_general(left, right, (((0,), (0,)), ((), ())), preferred_element_type=F32)


def silu(v):
    return v * jax.nn.sigmoid(v)


def in_three(value):
    high = value.astype(BF16)
    rest = value - high.astype(F32)
    middle = rest.astype(BF16)
    low = (rest - middle.astype(F32)).astype(BF16)
    return high, middle, low


def diagonal():
    return lax.broadcasted_iota(jnp.int32, (W, W), 0) == lax.broadcasted_iota(jnp.int32, (W, W), 1)


def to_column(row):
    eye = diagonal()
    return jnp.concatenate(
        [
            jnp.sum(jnp.where(eye, row[:, k * W : (k + 1) * W], 0.0), axis=1, keepdims=True)
            for k in range(row.shape[1] // W)
        ],
        axis=0,
    )


def to_row(column):
    eye = diagonal()
    return jnp.concatenate(
        [
            jnp.sum(jnp.where(eye, column[k * W : (k + 1) * W], 0.0), axis=0, keepdims=True)
            for k in range(column.shape[0] // W)
        ],
        axis=1,
    )


def kernel(
    zs,
    forget_hbm,
    value_hbm,
    gap_hbm,
    query_hbm,
    gatep_hbm,
    head_gain_hbm,
    ids_hbm,
    eg_hbm,
    stream_hbm,
    norm_gain_hbm,
    weights_hbm,
    proj_hbm,
    eu_hbm,
    sg_hbm,
    su_hbm,
    sd_hbm,
    ed_hbm,
    out_hbm,
    forget_ref,
    value_ref,
    gap_ref,
    query_ref,
    gatep_ref,
    head_gain_ref,
    ids_ref,
    stream_ref,
    norm_gain_ref,
    weights_ref,
    out_ref,
    wo,
    wsg,
    wsu,
    wsd,
    weg,
    weu,
    wed,
    pair_mine,
    pair_other,
    near_send,
    near_recv,
    near_decay,
    near_decays,
    far_send,
    far_recv,
    far_decay,
    far_decays,
    half_mine,
    half_other,
    squares,
    x_mixed,
    x_normed,
    x_shared,
    x_rows,
    x_hidden,
    send_rows,
    recv_rows,
    result,
    gathered,
    back,
    choose,
    pick0,
    pick1,
    residual,
    total_out,
    within,
    carried,
    gate_act,
    slots,
    sems,
):
    z, c = lax.axis_index("z"), lax.axis_index("c")
    y, x = lax.axis_index("y"), lax.axis_index("x")
    me = z * 2 + c
    spn = zs * 2
    j = y * 4 + x
    a = x * (1 - c) + y * c
    b = y * (1 - c) + x * c
    chunk = spn * CH
    group = chunk // 4

    def plane(a_to, b_to):
        return (z, c, b_to * (1 - c) + a_to * c, a_to * (1 - c) + b_to * c)

    def number(a_to, b_to):
        return (b_to * (1 - c) + a_to * c) * 4 + a_to * (1 - c) + b_to * c

    def column(number_of):
        return pl.ds(pl.multiple_of(number_of * W, W), W)

    def rows_of(number_of, count, base=0):
        return pl.ds(pl.multiple_of(base + number_of * count, count), count)

    def remote(src, dst, sent, received, where):
        return pltpu.make_async_remote_copy(
            src_ref=src,
            dst_ref=dst,
            send_sem=sems.at[sent],
            recv_sem=sems.at[received],
            device_id=where,
            device_id_type=MESH,
        )

    local = {}
    for k, (name, src, dst) in enumerate(
        [
            ("forget", forget_hbm, forget_ref),
            ("gap", gap_hbm, gap_ref),
            ("value", value_hbm, value_ref),
            ("query", query_hbm, query_ref),
            ("gatep", gatep_hbm, gatep_ref),
            ("head", head_gain_hbm, head_gain_ref),
            ("ids", ids_hbm, ids_ref),
            ("eg", eg_hbm, weg.at[:, column(a)]),
            ("stream", stream_hbm, stream_ref),
            ("gain", norm_gain_hbm, norm_gain_ref),
            ("routes", weights_hbm, weights_ref),
            ("wo", proj_hbm, wo),
            ("eu", eu_hbm, weu.at[:, column(a)]),
            ("sg", sg_hbm, wsg),
            ("su", su_hbm, wsu),
            ("sd", sd_hbm, wsd),
            ("ed", ed_hbm, wed.at[:, column(a)]),
        ]
    ):
        local[name] = pltpu.make_async_copy(src, dst, sems.at[INPUTS + k])
        local[name].start()

    barrier = pltpu.get_barrier_semaphore()

    def greet_column(i, carry):
        to = (me + i) % spn
        pl.semaphore_signal(barrier, inc=1, device_id=(to // 2, to % 2, y, x), device_id_type=MESH)
        return carry

    def greet_plane(i, carry):
        to = (j + i) % 16
        pl.semaphore_signal(barrier, inc=1, device_id=(z, c, to // 4, to % 4), device_id_type=MESH)
        return carry

    lax.fori_loop(1, spn, greet_column, 0)
    lax.fori_loop(1, 16, greet_plane, 0)

    local["forget"].wait()
    local["gap"].wait()
    leakage = gap_ref[...] * jax.nn.sigmoid(-forget_ref[...].astype(F32))
    log_keep = jnp.log1p(-leakage)
    lower = (
        lax.broadcasted_iota(jnp.int32, (T, T), 0) >= lax.broadcasted_iota(jnp.int32, (T, T), 1)
    ).astype(BF16)
    high, middle, low = in_three(log_keep)
    growth = dot(lower, high) + dot(lower, middle) + dot(lower, low)
    closing = growth[T - 1 : T, :]
    local["value"].wait()
    values = value_ref[...]
    state = dot_first(values, (leakage * jnp.exp(closing - growth)).astype(BF16))
    through = jnp.exp(closing)
    pair_mine[0:W, :] = state
    pair_mine[W : W + 8, :] = jnp.broadcast_to(through, (8, W))

    pl.semaphore_wait(barrier, spn - 1 + 15)

    swap = remote(pair_mine, pair_other, PAIR, PAIR + 1, (z, 1 - c, y, x))
    swap.start()

    next_a, last_a = (a + 1) % 4, (a + 3) % 4
    pending = []

    def weight_copies(which, src, dst):
        sem = WEIGHTS[which]
        upper, lower_half, every = pl.ds(0, D // 2), pl.ds(D // 2, D // 2), pl.ds(0, D)

        def step(part, owner, to, kind, source=None):
            block = dst.at[part, column(owner)]
            return remote(source if source is not None else block, block, sem, sem + 1 + kind, plane(to, b))

        def begin():
            step(every, a, next_a, 0, src).start()
            step(every, a, last_a, 1, src).start()

        def forward():
            step(every, last_a, next_a, 0).wait_recv()
            step(upper, last_a, next_a, 2).start()
            step(every, next_a, last_a, 1).wait_recv()
            step(lower_half, next_a, last_a, 3).start()

        def finish():
            opposite = (a + 2) % 4
            step(upper, opposite, next_a, 2).wait_recv()
            step(lower_half, opposite, last_a, 3).wait_recv()
            sent = dst.at[:, pl.ds(0, 3 * W)]
            pending.append(remote(sent, sent, sem, sem + 1, plane(next_a, b)))

        return begin, forward, finish

    gate_begin, gate_forward, gate_finish = weight_copies(0, eg_hbm, weg)
    up_begin, up_forward, up_finish = weight_copies(1, eu_hbm, weu)
    down_begin, down_forward, down_finish = weight_copies(2, ed_hbm, wed)
    gate_begin()

    swap.wait_recv()
    other_state, other_through = pair_other[0:W, :], pair_other[W : W + 1, :]
    mine_first = c == 0
    first = jnp.where(mine_first, state, other_state)
    second = jnp.where(mine_first, other_state, state)
    second_through = jnp.where(mine_first, other_through, through)
    total = first * second_through + second
    mine_total = jnp.where(mine_first, total[0:CAP, :], total[CAP:W, :])
    mine_decay = through * other_through
    near_send[...] = mine_total.astype(BF16)
    near_decay[...] = mine_decay
    quad, spot = z // 4, z % 4

    def near_copies(to, slot):
        where = (quad * 4 + to, c, y, x)
        return (
            remote(near_send, near_recv.at[slot], NEAR_S + to, NEAR_R + slot, where),
            remote(near_decay, near_decays.at[slot], NEAR_S + 4 + to, NEAR_R + 4 + slot, where),
        )

    def far_copies(to, slot):
        where = (to, c, y, x)
        return (
            remote(far_send, far_recv.at[slot], STATE_S + to, STATE_R + slot, where),
            remote(far_decay, far_decays.at[slot], DECAY_S + to, DECAY_R + slot, where),
        )

    def send_near(to, carry):
        for copy in near_copies(to, spot):
            copy.start()
        return carry

    lax.fori_loop(spot + 1, 4, send_near, 0)

    local["query"].wait()
    local["gatep"].wait()
    local["head"].wait()
    queries = silu(query_ref[...].astype(F32))
    centre = growth[T // 2 - 1 : T // 2, :]
    scaled_q = (queries * jnp.exp(growth - centre)).astype(BF16)
    scaled_k = (leakage * jnp.exp(centre - growth)).astype(BF16)
    carried[...] = (queries * jnp.exp(growth)).astype(BF16)
    gate_act[...] = silu(gatep_ref[...].astype(F32)) * head_gain_ref[...]
    for k in range(T // W):
        upto = (k + 1) * W
        scores = dot_last(scaled_q[k * W : upto, :], scaled_k[0:upto, :])
        causal = lax.broadcasted_iota(jnp.int32, (W, upto), 0) + k * W >= lax.broadcasted_iota(
            jnp.int32, (W, upto), 1
        )
        scores = jnp.where(causal, scores, 0.0).astype(BF16)
        within[k * W : upto, :] = dot(scores, values[0:upto, :])

    local["ids"].wait()
    ids = ids_ref[...]
    lanes = lax.broadcasted_iota(jnp.int32, (W, T), 0)
    hits0, hits1 = lanes == ids[0:1, :], lanes == ids[1:2, :]
    before = (
        lax.broadcasted_iota(jnp.int32, (T, T), 0) < lax.broadcasted_iota(jnp.int32, (T, T), 1)
    ).astype(BF16)
    earlier = dot((hits0 | hits1).astype(BF16), before)
    place = earlier + lanes.astype(F32) * CH
    for h in range(1, CHUNKS):
        place += jnp.where(earlier >= h * CH, float(chunk - CH), 0.0)
    slot0 = jnp.sum(jnp.where(hits0, place, 0.0), axis=0, keepdims=True)
    slot1 = jnp.sum(jnp.where(hits1, place, 0.0), axis=0, keepdims=True)
    slots[0] = jnp.broadcast_to(to_column(slot0), (T, W))
    slots[1] = jnp.broadcast_to(to_column(slot1), (T, W))

    def build(i, carry):
        base = (i * W).astype(F32)
        down = lax.broadcasted_iota(jnp.int32, (W, T), 0).astype(F32) + base
        choose[rows_of(i, W), :] = ((down == slot0) | (down == slot1)).astype(BF16)
        along = lax.broadcasted_iota(jnp.int32, (T, W), 1).astype(F32) + base
        pick0[:, column(i)] = (slots[0] == along).astype(BF16)
        pick1[:, column(i)] = (slots[1] == along).astype(BF16)
        return carry

    lax.fori_loop(0, spn * CAP // W, build, 0)
    def take_near(k, held):
        for copy in near_copies(k, k):
            copy.wait_recv()
        return held[0] * near_decays[k] + near_recv[k].astype(F32), held[1] * near_decays[k]

    near, near_through = lax.fori_loop(
        0, spot, take_near, (jnp.zeros((CAP, W), F32), jnp.ones((1, W), F32))
    )
    far_send[...] = (near * near_decay[...] + mine_total).astype(BF16)
    far_decay[...] = near_through * near_decay[...]
    far_count = jnp.where(spot == 3, zs - 1 - z, 0)

    def send_far(i, carry):
        for copy in far_copies(zs - 1 - i, quad):
            copy.start()
        return carry

    lax.fori_loop(0, far_count, send_far, 0)
    gate_forward()
    up_begin()
    up_forward()

    def take_far(k, held):
        for copy in far_copies(k, k):
            copy.wait_recv()
        return held * far_decays[k] + far_recv[k].astype(F32)

    half = lax.fori_loop(0, quad, take_far, jnp.zeros((CAP, W), F32))
    half = half * near_through + near
    half_mine[...] = half
    swap_half = remote(half_mine, half_other, PAIR_H, PAIR_H + 1, (z, 1 - c, y, x))
    swap_half.start()
    swap_half.wait_recv()
    theirs = half_other[...]
    incoming = jnp.concatenate(
        [jnp.where(mine_first, half, theirs), jnp.where(mine_first, theirs, half)], axis=0
    )
    incoming = jnp.where(
        mine_first, incoming, incoming * pair_other[W : W + 1, :] + pair_other[0:W, :]
    )
    outputs = within[...] + dot_last(carried[...], incoming.astype(BF16))
    mean = jnp.mean(outputs * outputs, axis=1, keepdims=True)
    x_mixed[:, column(j)] = (outputs * lax.rsqrt(mean + EPS) * gate_act[...]).astype(BF16)

    def along_b(buffer, which, order):
        sem = ALONG_B[which]
        rows = buffer.shape[0]
        upper, lower_half, every = pl.ds(0, rows // 2), pl.ds(rows // 2, rows // 2), pl.ds(0, rows)
        right, left, opposite = (b + 1) % 4, (b + 3) % 4, (b + 2) % 4

        def step(i, part, b_of, to, kind):
            block = buffer.at[part, column(number((a + 4 - i) % 4, b_of))]
            return remote(block, block, sem, sem + 1 + 4 * kind + i, plane(a, to))

        def begin(i):
            step(i, every, b, right, 0).start()
            step(i, every, b, left, 1).start()

        def forward(i):
            step(i, every, left, right, 0).wait_recv()
            step(i, upper, left, right, 2).start()
            step(i, every, right, left, 1).wait_recv()
            step(i, lower_half, right, left, 3).start()

        def finish():
            for i in order:
                step(i, upper, opposite, right, 2).wait_recv()
                step(i, lower_half, opposite, left, 3).wait_recv()
            sent = buffer.at[:, pl.ds(0, 12 * W)]
            pending.append(remote(sent, sent, sem, sem + 1, plane(a, right)))

        return begin, forward, finish

    def send_along_a(which, source_of, target_of, from_block):
        sem = ALONG_A[which]
        for i in (1, 3, 2):
            to = (a + i) % 4
            remote(source_of(to), target_of(a), sem, sem + i, plane(to, b)).start()

        def ready(i):
            if i:
                block = target_of((a + 4 - i) % 4)
                remote(block, block, sem, sem + i, plane((a + i) % 4, b)).wait_recv()

        pending.append((sem, from_block))
        return ready

    def columns_of(buffer):
        return lambda number_a: buffer.at[:, column(number(number_a, b))]

    ORDER = (0, 1, 3, 2)

    def gather_begin(buffer, which):
        begin, forward, finish = along_b(buffer, which, ORDER)
        own = buffer.at[:, column(j)]
        ready = send_along_a(which, lambda to: own, columns_of(buffer), buffer.at[:, pl.ds(0, 3 * W)])
        begin(0)

        def rest():
            last = 0
            for i in ORDER[1:]:
                ready(i)
                begin(i)
                forward(last)
                last = i
            forward(last)

        return rest, finish

    mixed_rest, mixed_finish = gather_begin(x_mixed, 0)
    mixed_rest()
    mixed_finish()

    local["wo"].wait()
    local["stream"].wait()
    res = stream_ref[...].astype(F32) + dot(x_mixed[...], wo[...])
    residual[...] = res
    squares[j] = to_row(jnp.sum(res * res, axis=1, keepdims=True))

    def send_squares(i, carry):
        to = (j + i) % 16
        remote(squares.at[j], squares.at[j], SQUARE, SQUARE + 1, (z, c, to // 4, to % 4)).start()
        return carry

    lax.fori_loop(1, 16, send_squares, 0)
    fifteen = squares.at[pl.ds(0, 15)]
    all_squares = remote(fifteen, fifteen, SQUARE, SQUARE + 1, plane(next_a, b))
    all_squares.wait_recv()
    summed = jnp.sum(squares[...], axis=0)
    scale = to_column(lax.rsqrt(summed / D + EPS))
    local["gain"].wait()
    normed = (res * scale * norm_gain_ref[...]).astype(BF16)
    x_normed[:, column(j)] = normed

    def exchange(src, dst, pair, h):
        def send(i, carry):
            to = (me + i) % spn
            remote(
                src.at[rows_of(to, CH, h * chunk), :],
                dst.at[rows_of(me, CH, h * chunk), :],
                pair,
                pair + 1,
                (to // 2, to % 2, y, x),
            ).start()
            return carry

        lax.fori_loop(1, spn, send, 0)
        dst[rows_of(me, CH, h * chunk), :] = src[rows_of(me, CH, h * chunk), :]
        others = dst.at[pl.ds(h * chunk, chunk - CH), :]
        whole = remote(others, others, pair, pair + 1, (z, 1 - c, y, x))
        pending.append(whole)
        return whole.wait_recv

    arrived = []
    for h in range(CHUNKS):
        for k in range(chunk // T):
            part = slice(h * chunk + k * T, h * chunk + (k + 1) * T)
            send_rows[part, :] = dot(choose[part, :], normed).astype(BF16)
        arrived.append(exchange(send_rows, recv_rows, OUT[h], h))

    def rows_start(h):
        arrived[h]()
        own_rows = rows_of(a, group, h * chunk)
        x_rows[h, :, column(j)] = recv_rows[own_rows, :]
        return send_along_a(
            3 + h,
            lambda to: recv_rows.at[rows_of(to, group, h * chunk), :],
            columns_of(x_rows.at[h]),
            x_rows.at[h, :, pl.ds(0, 3 * W)],
        )

    def gate_up(h):
        step = min(group, 2 * W)
        for k in range(group // step):
            part = slice(k * step, (k + 1) * step)
            rows_in = x_rows[h, part, :]
            hidden = (silu(dot(rows_in, weg[...])) * dot(rows_in, weu[...])).astype(BF16)
            for n in range(4):
                x_hidden[h, part, column(number(n, b))] = hidden[:, n * W : (n + 1) * W]

    def down_back(h):
        step = min(group, 2 * W)
        for k in range(group // step):
            part = slice(k * step, (k + 1) * step)
            rows_out = dot(x_hidden[h, part, :], wed[...]).astype(BF16)
            for n in range(4):
                result[h, n, part, :] = rows_out[:, n * W : (n + 1) * W]
        ready = send_along_a(
            3 + CHUNKS + h,
            lambda to: result.at[h, to],
            lambda number_a: gathered.at[rows_of(number_a, group, h * chunk), :],
            gathered.at[pl.ds(h * chunk, 3 * group), :],
        )
        gathered[rows_of(a, group, h * chunk), :] = result[h, a]
        return ready

    rows_b = [along_b(x_rows.at[h], 3 + h, ORDER) for h in range(CHUNKS)]
    hidden_b = [along_b(x_hidden.at[h], 3 + CHUNKS + h, ORDER) for h in range(CHUNKS)]

    def rows_begin(h, ready):
        for i in ORDER:
            ready(i)
            rows_b[h][0](i)

    def each(function):
        for i in ORDER:
            function(i)

    def go_back(h, ready):
        for i in (1, 3, 2):
            ready(i)
        return exchange(gathered, back, BACK[h], h)

    normed_rest, normed_finish = gather_begin(x_normed, 1)
    normed_rest()
    ready0 = rows_start(0)
    down_begin()
    normed_finish()
    local["sg"].wait()
    local["su"].wait()
    hidden = silu(dot(x_normed[...], wsg[...])) * dot(x_normed[...], wsu[...])
    x_shared[:, column(j)] = hidden.astype(BF16)
    rows_begin(0, ready0)
    each(rows_b[0][1])
    down_forward()
    rows_b[0][2]()
    gate_finish()
    local["eg"].wait()
    up_finish()
    local["eu"].wait()
    gate_up(0)
    each(hidden_b[0][0])
    ready1 = rows_start(1)
    each(hidden_b[0][1])
    rows_begin(1, ready1)
    hidden_b[0][2]()
    down_finish()
    local["ed"].wait()
    back0 = down_back(0)
    each(rows_b[1][1])
    returned0 = go_back(0, back0)
    rows_b[1][2]()
    gate_up(1)
    each(hidden_b[1][0])
    shared_rest, shared_finish = gather_begin(x_shared, 2)
    each(hidden_b[1][1])
    hidden_b[1][2]()
    back1 = down_back(1)
    returned1 = go_back(1, back1)
    shared_rest()
    shared_finish()
    local["sd"].wait()
    local["routes"].wait()
    weights = weights_ref[...]
    weight0, weight1 = to_column(weights[0:1, :]), to_column(weights[1:2, :])
    total_out[...] = residual[...] + dot(x_shared[...], wsd[...])

    def routed(h):
        part = slice(h * chunk, (h + 1) * chunk)
        rows_in = back[part, :]
        return dot(pick0[:, part], rows_in) * weight0 + dot(pick1[:, part], rows_in) * weight1

    returned0()
    total_out[...] += routed(0)

    swap.wait_send()
    swap_half.wait_send()
    all_squares.wait_send()

    def drain_near(to, carry):
        for copy in near_copies(to, spot):
            copy.wait_send()
        return carry

    def drain_far(i, carry):
        for copy in far_copies(zs - 1 - i, quad):
            copy.wait_send()
        return carry

    lax.fori_loop(spot + 1, 4, drain_near, 0)
    lax.fori_loop(0, far_count, drain_far, 0)
    for item in pending:
        if isinstance(item, tuple):
            item = remote(item[1], item[1], item[0], item[0] + 1, plane(next_a, b))
        item.wait_send()

    returned1()
    out_ref[...] = (total_out[...] + routed(1)).astype(BF16)
    leave = pltpu.make_async_copy(out_ref, out_hbm, sems.at[OUTPUT])
    leave.start()
    leave.wait()


def layer(zs, *args):
    (
        query_pre,
        forget_pre,
        values_in,
        gate_pre,
        floor_gap,
        head_gain,
        stream,
        out_proj,
        norm_gain,
        route_ids,
        route_weights,
        expert_gate,
        expert_up,
        expert_down,
        shared_gate,
        shared_up,
        shared_down,
    ) = args
    rows = zs * 2 * CAP
    group = rows // (4 * CHUNKS)
    hbm = pl.BlockSpec(memory_space=pl.ANY)
    tokens = pltpu.VMEM((T, W), BF16)
    line = pltpu.VMEM((1, W), F32)
    scratch = [
        tokens,
        tokens,
        line,
        tokens,
        tokens,
        line,
        pltpu.VMEM((2, T), jnp.int32),
        tokens,
        line,
        pltpu.VMEM((2, T), F32),
        tokens,
        *[pltpu.VMEM((D, W), BF16)] * 4,
        *[pltpu.VMEM((D, 4 * W), BF16)] * 3,
        *[pltpu.VMEM((W + 8, W), F32)] * 2,
        *[
            pltpu.VMEM((CAP, W), BF16),
            pltpu.VMEM((4, CAP, W), BF16),
            line,
            pltpu.VMEM((4, 1, W), F32),
        ]
        * 2,
        *[pltpu.VMEM((CAP, W), F32)] * 2,
        pltpu.VMEM((16, 1, T), F32),
        *[pltpu.VMEM((T, D), BF16)] * 3,
        *[pltpu.VMEM((CHUNKS, group, D), BF16)] * 2,
        *[pltpu.VMEM((rows, W), BF16)] * 2,
        pltpu.VMEM((CHUNKS, 4, group, W), BF16),
        *[pltpu.VMEM((rows, W), BF16)] * 2,
        pltpu.VMEM((rows, T), BF16),
        *[pltpu.VMEM((T, rows), BF16)] * 2,
        *[pltpu.VMEM((T, W), F32)] * 3,
        tokens,
        pltpu.VMEM((T, W), F32),
        pltpu.VMEM((2, T, W), F32),
        pltpu.SemaphoreType.DMA((SEM.used,)),
    ]
    return pl.pallas_call(
        functools.partial(kernel, zs),
        out_shape=jax.ShapeDtypeStruct((T, W), BF16),
        in_specs=[hbm] * 17,
        out_specs=hbm,
        scratch_shapes=scratch,
        compiler_params=pltpu.CompilerParams(
            collective_id=0, has_side_effects=True, vmem_limit_bytes=60 * 1024 * 1024
        ),
        name="layer",
    )(
        forget_pre,
        values_in,
        floor_gap.reshape(1, W),
        query_pre,
        gate_pre,
        head_gain.reshape(1, W),
        route_ids.T,
        expert_gate.reshape(D, W),
        stream,
        norm_gain.reshape(1, W),
        route_weights.T,
        out_proj,
        expert_up.reshape(D, W),
        shared_gate,
        shared_up,
        shared_down,
        expert_down.reshape(D, W),
    )


def solution(mesh):
    zs = mesh.shape["sp"] // 2
    finer = Mesh(mesh.devices.reshape(zs, 2, 4, 4), ("z", "c", "y", "x"))
    sp, tp = ("z", "c"), ("y", "x")
    in_specs = (
        P(sp, tp),
        P(sp, tp),
        P(sp, tp),
        P(sp, tp),
        P(tp),
        P(),
        P(sp, tp),
        P(None, tp),
        P(tp),
        P(sp, None),
        P(sp, None),
        P(sp, None, tp),
        P(sp, None, tp),
        P(sp, None, tp),
        P(None, tp),
        P(None, tp),
        P(None, tp),
    )
    return jax.shard_map(
        functools.partial(layer, zs),
        mesh=finer,
        in_specs=in_specs,
        out_specs=P(sp, tp),
        check_vma=False,
    )
```

```python
import functools

import jax
import jax.numpy as jnp
from jax import lax
from jax.experimental import pallas as pl
from jax.experimental.pallas import tpu as pltpu
from jax.sharding import Mesh
from jax.sharding import PartitionSpec as P

D = 2048
T = 512
W = 128
CAP = 64
EPS = 1e-06
MESH = pl.DeviceIdType.MESH
F32 = jnp.float32
BF16 = jnp.bfloat16


class Sems:
    def __init__(self):
        self.used = 0

    def take(self, count):
        first = self.used
        self.used += count
        return first


SEM = Sems()
CHUNKS = 4
SPACING = 1
CH = CAP // CHUNKS
INPUTS = SEM.take(17)
OUTPUT = SEM.take(1)
WEIGHTS = [SEM.take(13) for _ in range(3)]
PAIR = SEM.take(2)
PAIR_H = SEM.take(2)
NEAR_S, NEAR_R = SEM.take(8), SEM.take(8)
STATE_S, STATE_R = SEM.take(16), SEM.take(4)
DECAY_S, DECAY_R = SEM.take(16), SEM.take(4)
SQUARE = SEM.take(2)
SCALE = SEM.take(2)
OUT = [SEM.take(2) for _ in range(CHUNKS)]
BACK = [SEM.take(2) for _ in range(CHUNKS)]
RING_A = [SEM.take(5) for _ in range(3)]
ALONG_A = [SEM.take(4) for _ in range(3 + 2 * CHUNKS)]
ALONG_B = [SEM.take(17) for _ in range(3 + 2 * CHUNKS)]


def dot(left, right):
    return jnp.dot(left, right, preferred_element_type=F32)


def dot_last(left, right):
    return lax.dot_general(left, right, (((1,), (1,)), ((), ())), preferred_element_type=F32)


def dot_first(left, right):
    return lax.dot_general(left, right, (((0,), (0,)), ((), ())), preferred_element_type=F32)


def silu(v):
    return v * jax.nn.sigmoid(v)


def in_three(value):
    high = value.astype(BF16)
    rest = value - high.astype(F32)
    middle = rest.astype(BF16)
    low = (rest - middle.astype(F32)).astype(BF16)
    return high, middle, low


def diagonal():
    return lax.broadcasted_iota(jnp.int32, (W, W), 0) == lax.broadcasted_iota(jnp.int32, (W, W), 1)


def to_column(row):
    eye = diagonal()
    return jnp.concatenate(
        [
            jnp.sum(jnp.where(eye, row[:, k * W : (k + 1) * W], 0.0), axis=1, keepdims=True)
            for k in range(row.shape[1] // W)
        ],
        axis=0,
    )


def to_row(column):
    eye = diagonal()
    return jnp.concatenate(
        [
            jnp.sum(jnp.where(eye, column[k * W : (k + 1) * W], 0.0), axis=0, keepdims=True)
            for k in range(column.shape[0] // W)
        ],
        axis=1,
    )


def kernel(
    zs,
    forget_hbm,
    value_hbm,
    gap_hbm,
    query_hbm,
    gatep_hbm,
    head_gain_hbm,
    ids_hbm,
    eg_hbm,
    stream_hbm,
    norm_gain_hbm,
    weights_hbm,
    proj_hbm,
    eu_hbm,
    sg_hbm,
    su_hbm,
    sd_hbm,
    ed_hbm,
    out_hbm,
    forget_ref,
    value_ref,
    gap_ref,
    query_ref,
    gatep_ref,
    head_gain_ref,
    ids_ref,
    stream_ref,
    norm_gain_ref,
    weights_ref,
    out_ref,
    wo,
    wsg,
    wsu,
    wsd,
    weg,
    weu,
    wed,
    pair_mine,
    pair_other,
    near_send,
    near_recv,
    near_decay,
    near_decays,
    far_send,
    far_recv,
    far_decay,
    far_decays,
    half_mine,
    half_other,
    squares,
    x_mixed,
    x_normed,
    x_shared,
    x_rows,
    x_hidden,
    send_rows,
    recv_rows,
    result,
    gathered,
    back,
    choose,
    pick0,
    pick1,
    residual,
    total_out,
    within,
    carried,
    gate_act,
    slots,
    ranks,
    scales_send,
    scales_recv,
    sems,
):
    z, c = lax.axis_index("z"), lax.axis_index("c")
    y, x = lax.axis_index("y"), lax.axis_index("x")
    me = z * 2 + c
    spn = zs * 2
    j = y * 4 + x
    a = x * (1 - c) + y * c
    b = y * (1 - c) + x * c
    chunk = spn * CH
    group = chunk // 4

    def plane(a_to, b_to):
        return (z, c, b_to * (1 - c) + a_to * c, a_to * (1 - c) + b_to * c)

    def number(a_to, b_to):
        return (b_to * (1 - c) + a_to * c) * 4 + a_to * (1 - c) + b_to * c

    def column(number_of):
        return pl.ds(pl.multiple_of(number_of * W, W), W)

    def rows_of(number_of, count, base=0):
        return pl.ds(pl.multiple_of(base + number_of * count, count), count)

    def remote(src, dst, sent, received, where):
        return pltpu.make_async_remote_copy(
            src_ref=src,
            dst_ref=dst,
            send_sem=sems.at[sent],
            recv_sem=sems.at[received],
            device_id=where,
            device_id_type=MESH,
        )

    local = {}
    for k, (name, src, dst) in enumerate(
        [
            ("forget", forget_hbm, forget_ref),
            ("gap", gap_hbm, gap_ref),
            ("value", value_hbm, value_ref),
            ("query", query_hbm, query_ref),
            ("gatep", gatep_hbm, gatep_ref),
            ("head", head_gain_hbm, head_gain_ref),
            ("ids", ids_hbm, ids_ref),
            ("eg", eg_hbm, weg.at[:, column(a)]),
            ("stream", stream_hbm, stream_ref),
            ("gain", norm_gain_hbm, norm_gain_ref),
            ("routes", weights_hbm, weights_ref),
            ("wo", proj_hbm, wo),
            ("eu", eu_hbm, weu.at[:, column(a)]),
            ("sg", sg_hbm, wsg),
            ("su", su_hbm, wsu),
            ("sd", sd_hbm, wsd),
            ("ed", ed_hbm, wed.at[:, column(a)]),
        ]
    ):
        local[name] = pltpu.make_async_copy(src, dst, sems.at[INPUTS + k])
        local[name].start()

    barrier = pltpu.get_barrier_semaphore()

    def greet_column(i, carry):
        to = (me + i) % spn
        pl.semaphore_signal(barrier, inc=1, device_id=(to // 2, to % 2, y, x), device_id_type=MESH)
        return carry

    def greet_plane(i, carry):
        to = (j + i) % 16
        pl.semaphore_signal(barrier, inc=1, device_id=(z, c, to // 4, to % 4), device_id_type=MESH)
        return carry

    lax.fori_loop(1, spn, greet_column, 0)
    lax.fori_loop(1, 16, greet_plane, 0)

    local["forget"].wait()
    local["gap"].wait()
    leakage = gap_ref[...] * jax.nn.sigmoid(-forget_ref[...].astype(F32))
    log_keep = jnp.log1p(-leakage)
    lower = (
        lax.broadcasted_iota(jnp.int32, (T, T), 0) >= lax.broadcasted_iota(jnp.int32, (T, T), 1)
    ).astype(BF16)
    high, middle, low = in_three(log_keep)
    growth = dot(lower, high) + dot(lower, middle) + dot(lower, low)
    closing = growth[T - 1 : T, :]
    local["value"].wait()
    values = value_ref[...]
    state = dot_first(values, (leakage * jnp.exp(closing - growth)).astype(BF16))
    through = jnp.exp(closing)
    pair_mine[0:W, :] = state
    pair_mine[W : W + 8, :] = jnp.broadcast_to(through, (8, W))

    pl.semaphore_wait(barrier, spn - 1 + 15)

    swap = remote(pair_mine, pair_other, PAIR, PAIR + 1, (z, 1 - c, y, x))
    swap.start()

    next_a, last_a = (a + 1) % 4, (a + 3) % 4
    pending = []
    PIECES = 4

    def weight_copies(which, src, dst):
        sem = WEIGHTS[which]

        def step(k, owner, to, slot, source=None):
            part = pl.ds(k * (D // PIECES), D // PIECES)
            block = dst.at[part, column(owner)]
            return remote(
                block if source is None else source.at[part, :], block, sem, sem + 1 + slot, plane(to, b)
            )

        def begin(*pieces):
            for k in pieces:
                step(k, a, next_a, k, src).start()
                step(k, a, last_a, 4 + k, src).start()

        def forward(*pieces):
            for k in pieces:
                owner, to, slot = (last_a, next_a, k) if k % 2 == 0 else (next_a, last_a, 4 + k)
                step(k, owner, to, slot).wait_recv()
                step(k, owner, to, 8 + k).start()

        def finish():
            opposite = (a + 2) % 4
            for k in range(PIECES):
                owner, to, slot = (next_a, last_a, 4 + k) if k % 2 == 0 else (last_a, next_a, k)
                step(k, owner, to, slot).wait_recv()
                step(k, opposite, owner, 8 + k).wait_recv()
            sent = dst.at[:, pl.ds(0, 3 * W)]
            pending.append(remote(sent, sent, sem, sem + 1, plane(next_a, b)))

        return begin, forward, finish

    gate_begin, gate_forward, gate_finish = weight_copies(0, eg_hbm, weg)
    up_begin, up_forward, up_finish = weight_copies(1, eu_hbm, weu)
    down_begin, down_forward, down_finish = weight_copies(2, ed_hbm, wed)
    gate_begin(0, 1, 2, 3)

    swap.wait_recv()
    other_state, other_through = pair_other[0:W, :], pair_other[W : W + 1, :]
    mine_first = c == 0
    first = jnp.where(mine_first, state, other_state)
    second = jnp.where(mine_first, other_state, state)
    second_through = jnp.where(mine_first, other_through, through)
    total = first * second_through + second
    mine_total = jnp.where(mine_first, total[0:CAP, :], total[CAP:W, :])
    mine_decay = through * other_through
    near_send[...] = mine_total.astype(BF16)
    near_decay[...] = mine_decay
    quad, spot = z // 4, z % 4

    def near_copies(to, slot):
        where = (quad * 4 + to, c, y, x)
        return (
            remote(near_send, near_recv.at[slot], NEAR_S + to, NEAR_R + slot, where),
            remote(near_decay, near_decays.at[slot], NEAR_S + 4 + to, NEAR_R + 4 + slot, where),
        )

    def far_copies(to, slot):
        where = (to, c, y, x)
        return (
            remote(far_send, far_recv.at[slot], STATE_S + to, STATE_R + slot, where),
            remote(far_decay, far_decays.at[slot], DECAY_S + to, DECAY_R + slot, where),
        )

    def send_near(to, carry):
        for copy in near_copies(to, spot):
            copy.start()
        return carry

    lax.fori_loop(spot + 1, 4, send_near, 0)

    local["query"].wait()
    local["gatep"].wait()
    local["head"].wait()
    queries = silu(query_ref[...].astype(F32))
    centre = growth[T // 2 - 1 : T // 2, :]
    scaled_q = (queries * jnp.exp(growth - centre)).astype(BF16)
    scaled_k = (leakage * jnp.exp(centre - growth)).astype(BF16)
    carried[...] = (queries * jnp.exp(growth)).astype(BF16)
    gate_act[...] = silu(gatep_ref[...].astype(F32)) * head_gain_ref[...]
    for k in range(T // W):
        upto = (k + 1) * W
        scores = dot_last(scaled_q[k * W : upto, :], scaled_k[0:upto, :])
        causal = lax.broadcasted_iota(jnp.int32, (W, upto), 0) + k * W >= lax.broadcasted_iota(
            jnp.int32, (W, upto), 1
        )
        scores = jnp.where(causal, scores, 0.0).astype(BF16)
        within[k * W : upto, :] = dot(scores, values[0:upto, :])

    local["ids"].wait()
    ids = ids_ref[...]
    lanes = lax.broadcasted_iota(jnp.int32, (W, T), 0)
    hits0, hits1 = lanes == ids[0:1, :], lanes == ids[1:2, :]
    before = (
        lax.broadcasted_iota(jnp.int32, (T, T), 0) < lax.broadcasted_iota(jnp.int32, (T, T), 1)
    ).astype(BF16)
    earlier = dot((hits0 | hits1).astype(BF16), before)
    place = earlier + lanes.astype(F32) * CH
    for h in range(1, CHUNKS):
        place += jnp.where(earlier >= h * CH, float(chunk - CH), 0.0)
    slot0 = jnp.sum(jnp.where(hits0, place, 0.0), axis=0, keepdims=True)
    slot1 = jnp.sum(jnp.where(hits1, place, 0.0), axis=0, keepdims=True)
    among = lax.broadcasted_iota(jnp.int32, (T, W), 1).astype(F32)
    for k, hits in enumerate((hits0, hits1)):
        rank = jnp.sum(jnp.where(hits, earlier, 0.0), axis=0, keepdims=True)
        ranks[k] = (to_column(rank) == among).astype(BF16)
    slots[0] = jnp.broadcast_to(to_column(slot0), (T, W))
    slots[1] = jnp.broadcast_to(to_column(slot1), (T, W))

    def build(i, carry):
        base = (i * W).astype(F32)
        down = lax.broadcasted_iota(jnp.int32, (W, T), 0).astype(F32) + base
        choose[rows_of(i, W), :] = ((down == slot0) | (down == slot1)).astype(BF16)
        along = lax.broadcasted_iota(jnp.int32, (T, W), 1).astype(F32) + base
        pick0[:, column(i)] = (slots[0] == along).astype(BF16)
        pick1[:, column(i)] = (slots[1] == along).astype(BF16)
        return carry

    lax.fori_loop(0, spn * CAP // W, build, 0)
    def take_near(k, held):
        for copy in near_copies(k, k):
            copy.wait_recv()
        return held[0] * near_decays[k] + near_recv[k].astype(F32), held[1] * near_decays[k]

    near, near_through = lax.fori_loop(
        0, spot, take_near, (jnp.zeros((CAP, W), F32), jnp.ones((1, W), F32))
    )
    far_send[...] = (near * near_decay[...] + mine_total).astype(BF16)
    far_decay[...] = near_through * near_decay[...]
    far_count = jnp.where(spot == 3, zs - 1 - z, 0)

    def send_far(i, carry):
        for copy in far_copies(zs - 1 - i, quad):
            copy.start()
        return carry

    lax.fori_loop(0, far_count, send_far, 0)
    gate_forward(0, 1, 2, 3)
    up_begin(0, 1)

    def take_far(k, held):
        for copy in far_copies(k, k):
            copy.wait_recv()
        return held * far_decays[k] + far_recv[k].astype(F32)

    half = lax.fori_loop(0, quad, take_far, jnp.zeros((CAP, W), F32))
    half = half * near_through + near
    half_mine[...] = half
    swap_half = remote(half_mine, half_other, PAIR_H, PAIR_H + 1, (z, 1 - c, y, x))
    swap_half.start()
    swap_half.wait_recv()
    theirs = half_other[...]
    incoming = jnp.concatenate(
        [jnp.where(mine_first, half, theirs), jnp.where(mine_first, theirs, half)], axis=0
    )
    incoming = jnp.where(
        mine_first, incoming, incoming * pair_other[W : W + 1, :] + pair_other[0:W, :]
    )
    outputs = within[...] + dot_last(carried[...], incoming.astype(BF16))
    mean = jnp.mean(outputs * outputs, axis=1, keepdims=True)
    x_mixed[:, column(j)] = (outputs * lax.rsqrt(mean + EPS) * gate_act[...]).astype(BF16)

    def along_b(buffer, which, order):
        sem = ALONG_B[which]
        rows = buffer.shape[0]
        upper, lower_half, every = pl.ds(0, rows // 2), pl.ds(rows // 2, rows // 2), pl.ds(0, rows)
        right, left, opposite = (b + 1) % 4, (b + 3) % 4, (b + 2) % 4

        def step(i, part, b_of, to, kind):
            block = buffer.at[part, column(number((a + 4 - i) % 4, b_of))]
            return remote(block, block, sem, sem + 1 + 4 * kind + i, plane(a, to))

        def begin(i):
            step(i, every, b, right, 0).start()
            step(i, every, b, left, 1).start()

        def forward(i):
            step(i, every, left, right, 0).wait_recv()
            step(i, upper, left, right, 2).start()
            step(i, every, right, left, 1).wait_recv()
            step(i, lower_half, right, left, 3).start()

        def finish():
            for i in order:
                step(i, upper, opposite, right, 2).wait_recv()
                step(i, lower_half, opposite, left, 3).wait_recv()
            sent = buffer.at[:, pl.ds(0, 12 * W)]
            pending.append(remote(sent, sent, sem, sem + 1, plane(a, right)))

        return begin, forward, finish

    def send_along_a(which, source_of, target_of, from_block):
        sem = ALONG_A[which]
        for i in (1, 3, 2):
            to = (a + i) % 4
            remote(source_of(to), target_of(a), sem, sem + i, plane(to, b)).start()

        def ready(i):
            if i:
                block = target_of((a + 4 - i) % 4)
                remote(block, block, sem, sem + i, plane((a + i) % 4, b)).wait_recv()

        pending.append((sem, from_block))
        return ready

    def columns_of(buffer):
        return lambda number_a: buffer.at[:, column(number(number_a, b))]

    ORDER = (0, 1, 3, 2)

    def gather_begin(buffer, which):
        begin, forward, finish = along_b(buffer, which, ORDER)
        sem = RING_A[which]
        upper, lower_half, every = pl.ds(0, T // 2), pl.ds(T // 2, T // 2), pl.ds(0, T)

        def step(part, owner, to, kind):
            block = buffer.at[part, column(number(owner, b))]
            return remote(block, block, sem, sem + 1 + kind, plane(to, b))

        step(every, a, next_a, 0).start()
        step(every, a, last_a, 1).start()
        begin(0)

        def first():
            step(every, last_a, next_a, 0).wait_recv()
            step(upper, last_a, next_a, 2).start()
            begin(1)
            step(every, next_a, last_a, 1).wait_recv()
            step(lower_half, next_a, last_a, 3).start()
            begin(3)

        def second():
            forward(0)
            opposite = (a + 2) % 4
            step(upper, opposite, next_a, 2).wait_recv()
            step(lower_half, opposite, last_a, 3).wait_recv()
            begin(2)

        def third():
            forward(1)
            forward(3)
            forward(2)
            pending.append((sem, buffer.at[:, pl.ds(0, 3 * W)]))

        return first, second, third, finish

    for part in gather_begin(x_mixed, 0):
        part()

    local["wo"].wait()
    local["stream"].wait()
    res = stream_ref[...].astype(F32) + dot(x_mixed[...], wo[...])
    residual[...] = res
    squares[j] = to_row(jnp.sum(res * res, axis=1, keepdims=True))

    def send_squares(i, carry):
        to = (j + i) % 16
        remote(squares.at[j], squares.at[j], SQUARE, SQUARE + 1, (z, c, to // 4, to % 4)).start()
        return carry

    lax.fori_loop(1, 16, send_squares, 0)
    local["gain"].wait()
    normed = (res * norm_gain_ref[...]).astype(BF16)
    x_normed[:, column(j)] = normed
    up_begin(2, 3)

    def exchange(src, dst, pair, h):
        def send(n, carry):
            to = (me + spn // 2 + (n + 1) // 2 * (n % 2 * 2 - 1)) % spn
            remote(
                src.at[rows_of(to, CH, h * chunk), :],
                dst.at[rows_of(me, CH, h * chunk), :],
                pair,
                pair + 1,
                (to // 2, to % 2, y, x),
            ).start()
            return carry

        lax.fori_loop(0, spn - 1, send, 0)
        dst[rows_of(me, CH, h * chunk), :] = src[rows_of(me, CH, h * chunk), :]
        others = dst.at[pl.ds(h * chunk, chunk - CH), :]
        whole = remote(others, others, pair, pair + 1, (z, 1 - c, y, x))
        pending.append(whole)
        return whole.wait_recv

    arrived = []

    def dispatch(h):
        part = slice(h * chunk, (h + 1) * chunk)
        send_rows[part, :] = dot(choose[part, :], normed).astype(BF16)
        arrived.append(exchange(send_rows, recv_rows, OUT[h], h))

    dispatch(0)

    fifteen = squares.at[pl.ds(0, 15)]
    all_squares = remote(fifteen, fifteen, SQUARE, SQUARE + 1, plane(next_a, b))
    all_squares.wait_recv()
    factor = lax.rsqrt(jnp.sum(squares[...], axis=0) / D + EPS)
    experts = lax.broadcasted_iota(jnp.int32, (spn, T), 0)
    by_rank = jnp.zeros((spn, W), F32)
    for k in range(2):
        for piece in in_three(jnp.where(experts == ids_ref[k : k + 1, :], factor, 0.0)):
            by_rank += dot(piece, ranks[k])
    for k in range(spn):
        scales_send[k] = by_rank[k : k + 1, :]

    def send_scales(i, carry):
        to = (me + i) % spn
        remote(
            scales_send.at[to], scales_recv.at[me], SCALE, SCALE + 1, (to // 2, to % 2, y, x)
        ).start()
        return carry

    lax.fori_loop(1, spn, send_scales, 0)
    scales_recv[me] = scales_send[me]
    others = scales_recv.at[pl.ds(0, spn - 1)]
    all_scales = remote(others, others, SCALE, SCALE + 1, (z, 1 - c, y, x))
    pending.append(all_scales)
    dispatch(1)

    up_forward(0, 1, 2, 3)
    dispatch(2)
    dispatch(3)
    down_begin(0, 1)
    scale = to_column(factor)
    local["routes"].wait()
    weights = weights_ref[...]
    weight0, weight1 = to_column(weights[0:1, :]), to_column(weights[1:2, :])
    side = []

    def normed_start():
        side[0:0] = gather_begin(x_normed, 1)

    side.append(normed_start)

    def shared_hidden():
        local["sg"].wait()
        local["su"].wait()
        rows_in = x_normed[...]
        hidden = silu(dot(rows_in, wsg[...]) * scale) * (dot(rows_in, wsu[...]) * scale)
        x_shared[:, column(j)] = hidden.astype(BF16)
        side.extend(gather_begin(x_shared, 2))

    side.append(shared_hidden)

    def rows_start(h):
        arrived[h]()
        own_rows = rows_of(a, group, h * chunk)
        x_rows[h, :, column(j)] = recv_rows[own_rows, :]
        return send_along_a(
            3 + h,
            lambda to: recv_rows.at[rows_of(to, group, h * chunk), :],
            columns_of(x_rows.at[h]),
            x_rows.at[h, :, pl.ds(0, 3 * W)],
        )

    def gate_up(h):
        lane = lax.broadcasted_iota(jnp.int32, (CH, W), 1)
        place_of = lax.broadcasted_iota(jnp.int32, (CH, W), 0) + h * CH
        factors = jnp.concatenate(
            [
                jnp.sum(
                    jnp.where(lane == place_of, scales_recv[a * (spn // 4) + k], 0.0), axis=1, keepdims=True
                )
                for k in range(spn // 4)
            ],
            axis=0,
        )
        rows_in = x_rows[h]
        hidden = silu(dot(rows_in, weg[...]) * factors) * (dot(rows_in, weu[...]) * factors)
        hidden = hidden.astype(BF16)
        for n in range(4):
            x_hidden[h, :, column(number(n, b))] = hidden[:, n * W : (n + 1) * W]

    def down_back(h):
        step = min(group, 2 * W)
        for k in range(group // step):
            part = slice(k * step, (k + 1) * step)
            rows_out = dot(x_hidden[h, part, :], wed[...]).astype(BF16)
            for n in range(4):
                result[h, n, part, :] = rows_out[:, n * W : (n + 1) * W]
        ready = send_along_a(
            3 + CHUNKS + h,
            lambda to: result.at[h, to],
            lambda number_a: gathered.at[rows_of(number_a, group, h * chunk), :],
            gathered.at[pl.ds(h * chunk, 3 * group), :],
        )
        gathered[rows_of(a, group, h * chunk), :] = result[h, a]
        return ready

    rows_b = [along_b(x_rows.at[h], 3 + h, ORDER) for h in range(CHUNKS)]
    hidden_b = [along_b(x_hidden.at[h], 3 + CHUNKS + h, ORDER) for h in range(CHUNKS)]

    def rows_begin(h, ready):
        for i in ORDER:
            ready(i)
            rows_b[h][0](i)

    def each(function):
        for i in ORDER:
            function(i)

    def go_back(h, ready):
        for i in (1, 3, 2):
            ready(i)
        return exchange(gathered, back, BACK[h], h)

    held = {}

    def start_rows(h):
        held[h] = rows_start(h)
        if h == 0:
            down_begin(2)

    def begin_rows(h):
        rows_begin(h, held[h])
        if h == 0:
            down_begin(3)
            down_forward(0, 1)

    def forward_rows(h):
        each(rows_b[h][1])
        if h == 0:
            down_forward(2, 3)

    def through_gate(h):
        rows_b[h][2]()
        if h == 0:
            gate_finish()
            local["eg"].wait()
            up_finish()
            local["eu"].wait()
            all_scales.wait_recv()
        gate_up(h)
        each(hidden_b[h][0])

    def forward_hidden(h):
        each(hidden_b[h][1])

    def through_down(h):
        hidden_b[h][2]()
        if h == 0:
            down_finish()
            local["ed"].wait()
        held[h] = down_back(h)

    def send_home(h):
        held[h] = go_back(h, held[h])

    steps = (start_rows, begin_rows, forward_rows, through_gate, forward_hidden, through_down, send_home)
    SIDE = (2, 4, 5, 6, 7, 8)
    for tick in range(SPACING * (CHUNKS - 1) + len(steps)):
        for h in range(CHUNKS):
            at = tick - SPACING * h
            if 0 <= at < len(steps):
                steps[at](h)
        for _ in range(SIDE.count(tick)):
            side.pop(0)()

    while side:
        side.pop(0)()
    local["sd"].wait()
    total_out[...] = residual[...] + dot(x_shared[...], wsd[...])

    def routed(h):
        part = slice(h * chunk, (h + 1) * chunk)
        rows_in = back[part, :]
        return dot(pick0[:, part], rows_in) * weight0 + dot(pick1[:, part], rows_in) * weight1

    for h in range(CHUNKS - 1):
        held[h]()
        total_out[...] += routed(h)

    swap.wait_send()
    swap_half.wait_send()
    all_squares.wait_send()

    def drain_near(to, carry):
        for copy in near_copies(to, spot):
            copy.wait_send()
        return carry

    def drain_far(i, carry):
        for copy in far_copies(zs - 1 - i, quad):
            copy.wait_send()
        return carry

    lax.fori_loop(spot + 1, 4, drain_near, 0)
    lax.fori_loop(0, far_count, drain_far, 0)
    for item in pending:
        if isinstance(item, tuple):
            item = remote(item[1], item[1], item[0], item[0] + 1, plane(next_a, b))
        item.wait_send()

    held[CHUNKS - 1]()
    out_ref[...] = (total_out[...] + routed(CHUNKS - 1)).astype(BF16)
    leave = pltpu.make_async_copy(out_ref, out_hbm, sems.at[OUTPUT])
    leave.start()
    leave.wait()


def layer(zs, *args):
    (
        query_pre,
        forget_pre,
        values_in,
        gate_pre,
        floor_gap,
        head_gain,
        stream,
        out_proj,
        norm_gain,
        route_ids,
        route_weights,
        expert_gate,
        expert_up,
        expert_down,
        shared_gate,
        shared_up,
        shared_down,
    ) = args
    rows = zs * 2 * CAP
    group = rows // (4 * CHUNKS)
    hbm = pl.BlockSpec(memory_space=pl.ANY)
    tokens = pltpu.VMEM((T, W), BF16)
    line = pltpu.VMEM((1, W), F32)
    scratch = [
        tokens,
        tokens,
        line,
        tokens,
        tokens,
        line,
        pltpu.VMEM((2, T), jnp.int32),
        tokens,
        line,
        pltpu.VMEM((2, T), F32),
        tokens,
        *[pltpu.VMEM((D, W), BF16)] * 4,
        *[pltpu.VMEM((D, 4 * W), BF16)] * 3,
        *[pltpu.VMEM((W + 8, W), F32)] * 2,
        *[
            pltpu.VMEM((CAP, W), BF16),
            pltpu.VMEM((4, CAP, W), BF16),
            line,
            pltpu.VMEM((4, 1, W), F32),
        ]
        * 2,
        *[pltpu.VMEM((CAP, W), F32)] * 2,
        pltpu.VMEM((16, 1, T), F32),
        *[pltpu.VMEM((T, D), BF16)] * 3,
        *[pltpu.VMEM((CHUNKS, group, D), BF16)] * 2,
        *[pltpu.VMEM((rows, W), BF16)] * 2,
        pltpu.VMEM((CHUNKS, 4, group, W), BF16),
        *[pltpu.VMEM((rows, W), BF16)] * 2,
        pltpu.VMEM((rows, T), BF16),
        *[pltpu.VMEM((T, rows), BF16)] * 2,
        *[pltpu.VMEM((T, W), F32)] * 3,
        tokens,
        pltpu.VMEM((T, W), F32),
        pltpu.VMEM((2, T, W), F32),
        pltpu.VMEM((2, T, W), BF16),
        *[pltpu.VMEM((zs * 2, 1, W), F32)] * 2,
        pltpu.SemaphoreType.DMA((SEM.used,)),
    ]
    return pl.pallas_call(
        functools.partial(kernel, zs),
        out_shape=jax.ShapeDtypeStruct((T, W), BF16),
        in_specs=[hbm] * 17,
        out_specs=hbm,
        scratch_shapes=scratch,
        compiler_params=pltpu.CompilerParams(
            collective_id=0, has_side_effects=True, vmem_limit_bytes=60 * 1024 * 1024
        ),
        name="layer",
    )(
        forget_pre,
        values_in,
        floor_gap.reshape(1, W),
        query_pre,
        gate_pre,
        head_gain.reshape(1, W),
        route_ids.T,
        expert_gate.reshape(D, W),
        stream,
        norm_gain.reshape(1, W),
        route_weights.T,
        out_proj,
        expert_up.reshape(D, W),
        shared_gate,
        shared_up,
        shared_down,
        expert_down.reshape(D, W),
    )


def solution(mesh):
    zs = mesh.shape["sp"] // 2
    finer = Mesh(mesh.devices.reshape(zs, 2, 4, 4), ("z", "c", "y", "x"))
    sp, tp = ("z", "c"), ("y", "x")
    in_specs = (
        P(sp, tp),
        P(sp, tp),
        P(sp, tp),
        P(sp, tp),
        P(tp),
        P(),
        P(sp, tp),
        P(None, tp),
        P(tp),
        P(sp, None),
        P(sp, None),
        P(sp, None, tp),
        P(sp, None, tp),
        P(sp, None, tp),
        P(None, tp),
        P(None, tp),
        P(None, tp),
    )
    return jax.shard_map(
        functools.partial(layer, zs),
        mesh=finer,
        in_specs=in_specs,
        out_specs=P(sp, tp),
        check_vma=False,
    )
```

```python
import functools

import jax
import jax.numpy as jnp
from jax import lax
from jax.experimental import pallas as pl
from jax.experimental.pallas import tpu as pltpu
from jax.sharding import Mesh
from jax.sharding import PartitionSpec as P

D = 2048
T = 512
W = 128
CAP = 64
EPS = 1e-06
MESH = pl.DeviceIdType.MESH
F32 = jnp.float32
BF16 = jnp.bfloat16


class Sems:
    def __init__(self):
        self.used = 0

    def take(self, count):
        first = self.used
        self.used += count
        return first


SEM = Sems()
CHUNKS = 4
SPACING = 1
CH = CAP // CHUNKS
INPUTS = SEM.take(17)
OUTPUT = SEM.take(1)
WEIGHTS = [SEM.take(13) for _ in range(3)]
PAIR = SEM.take(2)
PAIR_H = SEM.take(2)
NEAR_S, NEAR_R = SEM.take(8), SEM.take(8)
STATE_S, STATE_R = SEM.take(16), SEM.take(4)
DECAY_S, DECAY_R = SEM.take(16), SEM.take(4)
SQUARE = SEM.take(2)
SCALE = SEM.take(2)
OUT = [SEM.take(2) for _ in range(CHUNKS)]
BACK = [SEM.take(2) for _ in range(CHUNKS)]
RING_A = [SEM.take(5) for _ in range(3)]
ALONG_A = [SEM.take(4) for _ in range(3 + 2 * CHUNKS)]
ALONG_B = [SEM.take(17) for _ in range(3 + 2 * CHUNKS)]


def dot(left, right):
    return jnp.dot(left, right, preferred_element_type=F32)


def dot_last(left, right):
    return lax.dot_general(left, right, (((1,), (1,)), ((), ())), preferred_element_type=F32)


def dot_first(left, right):
    return lax.dot_general(left, right, (((0,), (0,)), ((), ())), preferred_element_type=F32)


def silu(v):
    return v * jax.nn.sigmoid(v)


def in_three(value):
    high = value.astype(BF16)
    rest = value - high.astype(F32)
    middle = rest.astype(BF16)
    low = (rest - middle.astype(F32)).astype(BF16)
    return high, middle, low


def diagonal():
    return lax.broadcasted_iota(jnp.int32, (W, W), 0) == lax.broadcasted_iota(jnp.int32, (W, W), 1)


def to_column(row):
    eye = diagonal()
    return jnp.concatenate(
        [
            jnp.sum(jnp.where(eye, row[:, k * W : (k + 1) * W], 0.0), axis=1, keepdims=True)
            for k in range(row.shape[1] // W)
        ],
        axis=0,
    )


def to_row(column):
    eye = diagonal()
    return jnp.concatenate(
        [
            jnp.sum(jnp.where(eye, column[k * W : (k + 1) * W], 0.0), axis=0, keepdims=True)
            for k in range(column.shape[0] // W)
        ],
        axis=1,
    )


def kernel(
    zs,
    forget_hbm,
    value_hbm,
    gap_hbm,
    query_hbm,
    gatep_hbm,
    head_gain_hbm,
    ids_hbm,
    eg_hbm,
    stream_hbm,
    norm_gain_hbm,
    weights_hbm,
    proj_hbm,
    eu_hbm,
    sg_hbm,
    su_hbm,
    sd_hbm,
    ed_hbm,
    out_hbm,
    forget_ref,
    value_ref,
    gap_ref,
    query_ref,
    gatep_ref,
    head_gain_ref,
    ids_ref,
    stream_ref,
    norm_gain_ref,
    weights_ref,
    out_ref,
    wo,
    wsg,
    wsu,
    wsd,
    weg,
    weu,
    wed,
    pair_mine,
    pair_other,
    near_send,
    near_recv,
    near_decay,
    near_decays,
    far_send,
    far_recv,
    far_decay,
    far_decays,
    half_mine,
    half_other,
    squares,
    x_mixed,
    x_normed,
    x_shared,
    x_rows,
    x_hidden,
    send_rows,
    recv_rows,
    result,
    gathered,
    back,
    choose,
    pick0,
    pick1,
    residual,
    total_out,
    within,
    carried,
    gate_act,
    slots,
    ranks,
    scales_send,
    scales_recv,
    sems,
):
    z, c = lax.axis_index("z"), lax.axis_index("c")
    y, x = lax.axis_index("y"), lax.axis_index("x")
    me = z * 2 + c
    spn = zs * 2
    j = y * 4 + x
    a = x * (1 - c) + y * c
    b = y * (1 - c) + x * c
    chunk = spn * CH
    group = chunk // 4

    def plane(a_to, b_to):
        return (z, c, b_to * (1 - c) + a_to * c, a_to * (1 - c) + b_to * c)

    def number(a_to, b_to):
        return (b_to * (1 - c) + a_to * c) * 4 + a_to * (1 - c) + b_to * c

    def column(number_of):
        return pl.ds(pl.multiple_of(number_of * W, W), W)

    def rows_of(number_of, count, base=0):
        return pl.ds(pl.multiple_of(base + number_of * count, count), count)

    def remote(src, dst, sent, received, where):
        return pltpu.make_async_remote_copy(
            src_ref=src,
            dst_ref=dst,
            send_sem=sems.at[sent],
            recv_sem=sems.at[received],
            device_id=where,
            device_id_type=MESH,
        )

    local = {}
    for k, (name, src, dst) in enumerate(
        [
            ("forget", forget_hbm, forget_ref),
            ("gap", gap_hbm, gap_ref),
            ("value", value_hbm, value_ref),
            ("query", query_hbm, query_ref),
            ("gatep", gatep_hbm, gatep_ref),
            ("head", head_gain_hbm, head_gain_ref),
            ("ids", ids_hbm, ids_ref),
            ("eg", eg_hbm, weg.at[:, column(a)]),
            ("stream", stream_hbm, stream_ref),
            ("gain", norm_gain_hbm, norm_gain_ref),
            ("routes", weights_hbm, weights_ref),
            ("wo", proj_hbm, wo),
            ("eu", eu_hbm, weu.at[:, column(a)]),
            ("sg", sg_hbm, wsg),
            ("su", su_hbm, wsu),
            ("sd", sd_hbm, wsd),
            ("ed", ed_hbm, wed.at[:, column(a)]),
        ]
    ):
        local[name] = pltpu.make_async_copy(src, dst, sems.at[INPUTS + k])
        local[name].start()

    barrier = pltpu.get_barrier_semaphore()

    def greet_column(i, carry):
        to = (me + i) % spn
        pl.semaphore_signal(barrier, inc=1, device_id=(to // 2, to % 2, y, x), device_id_type=MESH)
        return carry

    def greet_plane(i, carry):
        to = (j + i) % 16
        pl.semaphore_signal(barrier, inc=1, device_id=(z, c, to // 4, to % 4), device_id_type=MESH)
        return carry

    lax.fori_loop(1, spn, greet_column, 0)
    lax.fori_loop(1, 16, greet_plane, 0)

    local["forget"].wait()
    local["gap"].wait()
    leakage = gap_ref[...] * jax.nn.sigmoid(-forget_ref[...].astype(F32))
    log_keep = jnp.log1p(-leakage)
    lower = (
        lax.broadcasted_iota(jnp.int32, (T, T), 0) >= lax.broadcasted_iota(jnp.int32, (T, T), 1)
    ).astype(BF16)
    high, middle, low = in_three(log_keep)
    growth = dot(lower, high) + dot(lower, middle) + dot(lower, low)
    closing = growth[T - 1 : T, :]
    local["value"].wait()
    values = value_ref[...]
    state = dot_first(values, (leakage * jnp.exp(closing - growth)).astype(BF16))
    through = jnp.exp(closing)
    pair_mine[0:W, :] = state
    pair_mine[W : W + 8, :] = jnp.broadcast_to(through, (8, W))

    pl.semaphore_wait(barrier, spn - 1 + 15)

    swap = remote(pair_mine, pair_other, PAIR, PAIR + 1, (z, 1 - c, y, x))
    swap.start()

    next_a, last_a = (a + 1) % 4, (a + 3) % 4
    pending = []
    PIECES = 4

    def weight_copies(which, src, dst):
        sem = WEIGHTS[which]

        def step(k, owner, to, slot, source=None):
            part = pl.ds(k * (D // PIECES), D // PIECES)
            block = dst.at[part, column(owner)]
            return remote(
                block if source is None else source.at[part, :], block, sem, sem + 1 + slot, plane(to, b)
            )

        def begin(*pieces):
            for k in pieces:
                step(k, a, next_a, k, src).start()
                step(k, a, last_a, 4 + k, src).start()

        def forward(*pieces):
            for k in pieces:
                owner, to, slot = (last_a, next_a, k) if k % 2 == 0 else (next_a, last_a, 4 + k)
                step(k, owner, to, slot).wait_recv()
                step(k, owner, to, 8 + k).start()

        def finish():
            opposite = (a + 2) % 4
            for k in range(PIECES):
                owner, to, slot = (next_a, last_a, 4 + k) if k % 2 == 0 else (last_a, next_a, k)
                step(k, owner, to, slot).wait_recv()
                step(k, opposite, owner, 8 + k).wait_recv()
            sent = dst.at[:, pl.ds(0, 3 * W)]
            pending.append(remote(sent, sent, sem, sem + 1, plane(next_a, b)))

        return begin, forward, finish

    gate_begin, gate_forward, gate_finish = weight_copies(0, eg_hbm, weg)
    up_begin, up_forward, up_finish = weight_copies(1, eu_hbm, weu)
    down_begin, down_forward, down_finish = weight_copies(2, ed_hbm, wed)
    gate_begin(0, 1, 2, 3)

    swap.wait_recv()
    other_state, other_through = pair_other[0:W, :], pair_other[W : W + 1, :]
    mine_first = c == 0
    first = jnp.where(mine_first, state, other_state)
    second = jnp.where(mine_first, other_state, state)
    second_through = jnp.where(mine_first, other_through, through)
    total = first * second_through + second
    mine_total = jnp.where(mine_first, total[0:CAP, :], total[CAP:W, :])
    mine_decay = through * other_through
    near_send[...] = mine_total.astype(BF16)
    near_decay[...] = mine_decay
    quad, spot = z // 4, z % 4

    def near_copies(to, slot):
        where = (quad * 4 + to, c, y, x)
        return (
            remote(near_send, near_recv.at[slot], NEAR_S + to, NEAR_R + slot, where),
            remote(near_decay, near_decays.at[slot], NEAR_S + 4 + to, NEAR_R + 4 + slot, where),
        )

    def far_copies(to, slot):
        where = (to, c, y, x)
        return (
            remote(far_send, far_recv.at[slot], STATE_S + to, STATE_R + slot, where),
            remote(far_decay, far_decays.at[slot], DECAY_S + to, DECAY_R + slot, where),
        )

    def send_near(to, carry):
        for copy in near_copies(to, spot):
            copy.start()
        return carry

    lax.fori_loop(spot + 1, 4, send_near, 0)

    local["query"].wait()
    local["gatep"].wait()
    local["head"].wait()
    queries = silu(query_ref[...].astype(F32))
    centre = growth[T // 2 - 1 : T // 2, :]
    scaled_q = (queries * jnp.exp(growth - centre)).astype(BF16)
    scaled_k = (leakage * jnp.exp(centre - growth)).astype(BF16)
    carried[...] = (queries * jnp.exp(growth)).astype(BF16)
    gate_act[...] = silu(gatep_ref[...].astype(F32)) * head_gain_ref[...]
    for k in range(T // W):
        upto = (k + 1) * W
        scores = dot_last(scaled_q[k * W : upto, :], scaled_k[0:upto, :])
        causal = lax.broadcasted_iota(jnp.int32, (W, upto), 0) + k * W >= lax.broadcasted_iota(
            jnp.int32, (W, upto), 1
        )
        scores = jnp.where(causal, scores, 0.0).astype(BF16)
        within[k * W : upto, :] = dot(scores, values[0:upto, :])

    local["ids"].wait()
    ids = ids_ref[...]
    lanes = lax.broadcasted_iota(jnp.int32, (W, T), 0)
    hits0, hits1 = lanes == ids[0:1, :], lanes == ids[1:2, :]
    before = (
        lax.broadcasted_iota(jnp.int32, (T, T), 0) < lax.broadcasted_iota(jnp.int32, (T, T), 1)
    ).astype(BF16)
    earlier = dot((hits0 | hits1).astype(BF16), before)
    place = earlier + lanes.astype(F32) * CH
    for h in range(1, CHUNKS):
        place += jnp.where(earlier >= h * CH, float(chunk - CH), 0.0)
    slot0 = jnp.sum(jnp.where(hits0, place, 0.0), axis=0, keepdims=True)
    slot1 = jnp.sum(jnp.where(hits1, place, 0.0), axis=0, keepdims=True)
    among = lax.broadcasted_iota(jnp.int32, (T, W), 1).astype(F32)
    for k, hits in enumerate((hits0, hits1)):
        rank = jnp.sum(jnp.where(hits, earlier, 0.0), axis=0, keepdims=True)
        ranks[k] = (to_column(rank) == among).astype(BF16)
    slots[0] = jnp.broadcast_to(to_column(slot0), (T, W))
    slots[1] = jnp.broadcast_to(to_column(slot1), (T, W))

    def build(i, carry):
        base = (i * W).astype(F32)
        down = lax.broadcasted_iota(jnp.int32, (W, T), 0).astype(F32) + base
        choose[rows_of(i, W), :] = ((down == slot0) | (down == slot1)).astype(BF16)
        along = lax.broadcasted_iota(jnp.int32, (T, W), 1).astype(F32) + base
        pick0[:, column(i)] = (slots[0] == along).astype(BF16)
        pick1[:, column(i)] = (slots[1] == along).astype(BF16)
        return carry

    lax.fori_loop(0, spn * CAP // W, build, 0)
    def take_near(k, held):
        for copy in near_copies(k, k):
            copy.wait_recv()
        return held[0] * near_decays[k] + near_recv[k].astype(F32), held[1] * near_decays[k]

    near, near_through = lax.fori_loop(
        0, spot, take_near, (jnp.zeros((CAP, W), F32), jnp.ones((1, W), F32))
    )
    far_send[...] = (near * near_decay[...] + mine_total).astype(BF16)
    far_decay[...] = near_through * near_decay[...]
    far_count = jnp.where(spot == 3, zs - 1 - z, 0)

    def send_far(i, carry):
        for copy in far_copies(zs - 1 - i, quad):
            copy.start()
        return carry

    lax.fori_loop(0, far_count, send_far, 0)
    gate_forward(0, 1, 2, 3)
    up_begin(0, 1)

    def take_far(k, held):
        for copy in far_copies(k, k):
            copy.wait_recv()
        return held * far_decays[k] + far_recv[k].astype(F32)

    half = lax.fori_loop(0, quad, take_far, jnp.zeros((CAP, W), F32))
    half = half * near_through + near
    half_mine[...] = half
    swap_half = remote(half_mine, half_other, PAIR_H, PAIR_H + 1, (z, 1 - c, y, x))
    swap_half.start()
    swap_half.wait_recv()
    theirs = half_other[...]
    incoming = jnp.concatenate(
        [jnp.where(mine_first, half, theirs), jnp.where(mine_first, theirs, half)], axis=0
    )
    incoming = jnp.where(
        mine_first, incoming, incoming * pair_other[W : W + 1, :] + pair_other[0:W, :]
    )
    outputs = within[...] + dot_last(carried[...], incoming.astype(BF16))
    mean = jnp.mean(outputs * outputs, axis=1, keepdims=True)
    x_mixed[:, column(j)] = (outputs * lax.rsqrt(mean + EPS) * gate_act[...]).astype(BF16)

    def along_b(buffer, which, order):
        sem = ALONG_B[which]
        rows = buffer.shape[0]
        upper, lower_half, every = pl.ds(0, rows // 2), pl.ds(rows // 2, rows // 2), pl.ds(0, rows)
        right, left, opposite = (b + 1) % 4, (b + 3) % 4, (b + 2) % 4

        def step(i, part, b_of, to, kind):
            block = buffer.at[part, column(number((a + 4 - i) % 4, b_of))]
            return remote(block, block, sem, sem + 1 + 4 * kind + i, plane(a, to))

        def begin(i):
            step(i, every, b, right, 0).start()
            step(i, every, b, left, 1).start()

        def forward(i):
            step(i, every, left, right, 0).wait_recv()
            step(i, upper, left, right, 2).start()
            step(i, every, right, left, 1).wait_recv()
            step(i, lower_half, right, left, 3).start()

        def finish():
            for i in order:
                step(i, upper, opposite, right, 2).wait_recv()
                step(i, lower_half, opposite, left, 3).wait_recv()
            sent = buffer.at[:, pl.ds(0, 12 * W)]
            pending.append(remote(sent, sent, sem, sem + 1, plane(a, right)))

        return begin, forward, finish

    def send_along_a(which, source_of, target_of, from_block):
        sem = ALONG_A[which]
        for i in (1, 3, 2):
            to = (a + i) % 4
            remote(source_of(to), target_of(a), sem, sem + i, plane(to, b)).start()

        def ready(i):
            if i:
                block = target_of((a + 4 - i) % 4)
                remote(block, block, sem, sem + i, plane((a + i) % 4, b)).wait_recv()

        pending.append((sem, from_block))
        return ready

    def columns_of(buffer):
        return lambda number_a: buffer.at[:, column(number(number_a, b))]

    ORDER = (0, 1, 3, 2)

    def gather_begin(buffer, which):
        begin, forward, finish = along_b(buffer, which, ORDER)
        sem = RING_A[which]
        upper, lower_half, every = pl.ds(0, T // 2), pl.ds(T // 2, T // 2), pl.ds(0, T)

        def step(part, owner, to, kind):
            block = buffer.at[part, column(number(owner, b))]
            return remote(block, block, sem, sem + 1 + kind, plane(to, b))

        step(every, a, next_a, 0).start()
        step(every, a, last_a, 1).start()
        begin(0)

        def first():
            step(every, last_a, next_a, 0).wait_recv()
            step(upper, last_a, next_a, 2).start()
            begin(1)
            step(every, next_a, last_a, 1).wait_recv()
            step(lower_half, next_a, last_a, 3).start()
            begin(3)

        def second():
            forward(0)
            opposite = (a + 2) % 4
            step(upper, opposite, next_a, 2).wait_recv()
            step(lower_half, opposite, last_a, 3).wait_recv()
            begin(2)

        def third():
            forward(1)
            forward(3)
            forward(2)
            pending.append((sem, buffer.at[:, pl.ds(0, 3 * W)]))

        return first, second, third, finish

    for part in gather_begin(x_mixed, 0):
        part()

    local["wo"].wait()
    local["stream"].wait()
    res = stream_ref[...].astype(F32) + dot(x_mixed[...], wo[...])
    residual[...] = res
    squares[j] = to_row(jnp.sum(res * res, axis=1, keepdims=True))

    def send_squares(i, carry):
        to = (j + i) % 16
        remote(squares.at[j], squares.at[j], SQUARE, SQUARE + 1, (z, c, to // 4, to % 4)).start()
        return carry

    lax.fori_loop(1, 16, send_squares, 0)
    local["gain"].wait()
    normed = (res * norm_gain_ref[...]).astype(BF16)
    x_normed[:, column(j)] = normed
    normed_parts = list(gather_begin(x_normed, 1))
    up_begin(2, 3)

    def exchange(src, dst, pair, h):
        def send(n, carry):
            to = (me + spn // 2 + (n + 1) // 2 * (n % 2 * 2 - 1)) % spn
            remote(
                src.at[rows_of(to, CH, h * chunk), :],
                dst.at[rows_of(me, CH, h * chunk), :],
                pair,
                pair + 1,
                (to // 2, to % 2, y, x),
            ).start()
            return carry

        lax.fori_loop(0, spn - 1, send, 0)
        dst[rows_of(me, CH, h * chunk), :] = src[rows_of(me, CH, h * chunk), :]
        others = dst.at[pl.ds(h * chunk, chunk - CH), :]
        whole = remote(others, others, pair, pair + 1, (z, 1 - c, y, x))
        pending.append(whole)
        return whole.wait_recv

    arrived = []

    def dispatch(h):
        part = slice(h * chunk, (h + 1) * chunk)
        send_rows[part, :] = dot(choose[part, :], normed).astype(BF16)
        arrived.append(exchange(send_rows, recv_rows, OUT[h], h))

    dispatch(0)

    fifteen = squares.at[pl.ds(0, 15)]
    all_squares = remote(fifteen, fifteen, SQUARE, SQUARE + 1, plane(next_a, b))
    all_squares.wait_recv()
    factor = lax.rsqrt(jnp.sum(squares[...], axis=0) / D + EPS)
    experts = lax.broadcasted_iota(jnp.int32, (spn, T), 0)
    by_rank = jnp.zeros((spn, W), F32)
    for k in range(2):
        for piece in in_three(jnp.where(experts == ids_ref[k : k + 1, :], factor, 0.0)):
            by_rank += dot(piece, ranks[k])
    for k in range(spn):
        scales_send[k] = by_rank[k : k + 1, :]

    def send_scales(i, carry):
        to = (me + i) % spn
        remote(
            scales_send.at[to], scales_recv.at[me], SCALE, SCALE + 1, (to // 2, to % 2, y, x)
        ).start()
        return carry

    lax.fori_loop(1, spn, send_scales, 0)
    scales_recv[me] = scales_send[me]
    others = scales_recv.at[pl.ds(0, spn - 1)]
    all_scales = remote(others, others, SCALE, SCALE + 1, (z, 1 - c, y, x))
    pending.append(all_scales)
    dispatch(1)

    normed_parts.pop(0)()
    up_forward(0, 1, 2, 3)
    dispatch(2)
    dispatch(3)
    normed_parts.pop(0)()
    down_begin(0, 1)
    scale = to_column(factor)
    local["routes"].wait()
    weights = weights_ref[...]
    weight0, weight1 = to_column(weights[0:1, :]), to_column(weights[1:2, :])
    side = normed_parts

    def shared_hidden():
        local["sg"].wait()
        local["su"].wait()
        rows_in = x_normed[...]
        hidden = silu(dot(rows_in, wsg[...]) * scale) * (dot(rows_in, wsu[...]) * scale)
        x_shared[:, column(j)] = hidden.astype(BF16)
        side.extend(gather_begin(x_shared, 2))

    side.append(shared_hidden)

    def rows_start(h):
        arrived[h]()
        own_rows = rows_of(a, group, h * chunk)
        x_rows[h, :, column(j)] = recv_rows[own_rows, :]
        return send_along_a(
            3 + h,
            lambda to: recv_rows.at[rows_of(to, group, h * chunk), :],
            columns_of(x_rows.at[h]),
            x_rows.at[h, :, pl.ds(0, 3 * W)],
        )

    def gate_up(h):
        lane = lax.broadcasted_iota(jnp.int32, (CH, W), 1)
        place_of = lax.broadcasted_iota(jnp.int32, (CH, W), 0) + h * CH
        factors = jnp.concatenate(
            [
                jnp.sum(
                    jnp.where(lane == place_of, scales_recv[a * (spn // 4) + k], 0.0), axis=1, keepdims=True
                )
                for k in range(spn // 4)
            ],
            axis=0,
        )
        rows_in = x_rows[h]
        hidden = silu(dot(rows_in, weg[...]) * factors) * (dot(rows_in, weu[...]) * factors)
        hidden = hidden.astype(BF16)
        for n in range(4):
            x_hidden[h, :, column(number(n, b))] = hidden[:, n * W : (n + 1) * W]

    def down_back(h):
        step = min(group, 2 * W)
        for k in range(group // step):
            part = slice(k * step, (k + 1) * step)
            rows_out = dot(x_hidden[h, part, :], wed[...]).astype(BF16)
            for n in range(4):
                result[h, n, part, :] = rows_out[:, n * W : (n + 1) * W]
        ready = send_along_a(
            3 + CHUNKS + h,
            lambda to: result.at[h, to],
            lambda number_a: gathered.at[rows_of(number_a, group, h * chunk), :],
            gathered.at[pl.ds(h * chunk, 3 * group), :],
        )
        gathered[rows_of(a, group, h * chunk), :] = result[h, a]
        return ready

    rows_b = [along_b(x_rows.at[h], 3 + h, ORDER) for h in range(CHUNKS)]
    hidden_b = [along_b(x_hidden.at[h], 3 + CHUNKS + h, ORDER) for h in range(CHUNKS)]

    def rows_begin(h, ready):
        for i in ORDER:
            ready(i)
            rows_b[h][0](i)

    def each(function):
        for i in ORDER:
            function(i)

    def go_back(h, ready):
        for i in (1, 3, 2):
            ready(i)
        return exchange(gathered, back, BACK[h], h)

    held = {}

    def start_rows(h):
        held[h] = rows_start(h)
        if h == 0:
            down_begin(2)

    def begin_rows(h):
        rows_begin(h, held[h])
        if h == 0:
            down_begin(3)
            down_forward(0, 1)

    def forward_rows(h):
        each(rows_b[h][1])
        if h == 0:
            down_forward(2, 3)

    def through_gate(h):
        rows_b[h][2]()
        if h == 0:
            gate_finish()
            local["eg"].wait()
            up_finish()
            local["eu"].wait()
            all_scales.wait_recv()
        gate_up(h)
        each(hidden_b[h][0])

    def forward_hidden(h):
        each(hidden_b[h][1])

    def through_down(h):
        hidden_b[h][2]()
        if h == 0:
            down_finish()
            local["ed"].wait()
        held[h] = down_back(h)

    def send_home(h):
        held[h] = go_back(h, held[h])

    steps = (start_rows, begin_rows, forward_rows, through_gate, forward_hidden, through_down, send_home)
    SIDE = (1, 2, 7, 8, 9)
    for tick in range(SPACING * (CHUNKS - 1) + len(steps)):
        for h in range(CHUNKS):
            at = tick - SPACING * h
            if 0 <= at < len(steps):
                steps[at](h)
        for _ in range(SIDE.count(tick)):
            side.pop(0)()

    while side:
        side.pop(0)()
    local["sd"].wait()
    total_out[...] = residual[...] + dot(x_shared[...], wsd[...])

    def routed(h):
        part = slice(h * chunk, (h + 1) * chunk)
        rows_in = back[part, :]
        return dot(pick0[:, part], rows_in) * weight0 + dot(pick1[:, part], rows_in) * weight1

    for h in range(CHUNKS - 1):
        held[h]()
        total_out[...] += routed(h)

    swap.wait_send()
    swap_half.wait_send()
    all_squares.wait_send()

    def drain_near(to, carry):
        for copy in near_copies(to, spot):
            copy.wait_send()
        return carry

    def drain_far(i, carry):
        for copy in far_copies(zs - 1 - i, quad):
            copy.wait_send()
        return carry

    lax.fori_loop(spot + 1, 4, drain_near, 0)
    lax.fori_loop(0, far_count, drain_far, 0)
    for item in pending:
        if isinstance(item, tuple):
            item = remote(item[1], item[1], item[0], item[0] + 1, plane(next_a, b))
        item.wait_send()

    held[CHUNKS - 1]()
    out_ref[...] = (total_out[...] + routed(CHUNKS - 1)).astype(BF16)
    leave = pltpu.make_async_copy(out_ref, out_hbm, sems.at[OUTPUT])
    leave.start()
    leave.wait()


def layer(zs, *args):
    (
        query_pre,
        forget_pre,
        values_in,
        gate_pre,
        floor_gap,
        head_gain,
        stream,
        out_proj,
        norm_gain,
        route_ids,
        route_weights,
        expert_gate,
        expert_up,
        expert_down,
        shared_gate,
        shared_up,
        shared_down,
    ) = args
    rows = zs * 2 * CAP
    group = rows // (4 * CHUNKS)
    hbm = pl.BlockSpec(memory_space=pl.ANY)
    tokens = pltpu.VMEM((T, W), BF16)
    line = pltpu.VMEM((1, W), F32)
    scratch = [
        tokens,
        tokens,
        line,
        tokens,
        tokens,
        line,
        pltpu.VMEM((2, T), jnp.int32),
        tokens,
        line,
        pltpu.VMEM((2, T), F32),
        tokens,
        *[pltpu.VMEM((D, W), BF16)] * 4,
        *[pltpu.VMEM((D, 4 * W), BF16)] * 3,
        *[pltpu.VMEM((W + 8, W), F32)] * 2,
        *[
            pltpu.VMEM((CAP, W), BF16),
            pltpu.VMEM((4, CAP, W), BF16),
            line,
            pltpu.VMEM((4, 1, W), F32),
        ]
        * 2,
        *[pltpu.VMEM((CAP, W), F32)] * 2,
        pltpu.VMEM((16, 1, T), F32),
        *[pltpu.VMEM((T, D), BF16)] * 3,
        *[pltpu.VMEM((CHUNKS, group, D), BF16)] * 2,
        *[pltpu.VMEM((rows, W), BF16)] * 2,
        pltpu.VMEM((CHUNKS, 4, group, W), BF16),
        *[pltpu.VMEM((rows, W), BF16)] * 2,
        pltpu.VMEM((rows, T), BF16),
        *[pltpu.VMEM((T, rows), BF16)] * 2,
        *[pltpu.VMEM((T, W), F32)] * 3,
        tokens,
        pltpu.VMEM((T, W), F32),
        pltpu.VMEM((2, T, W), F32),
        pltpu.VMEM((2, T, W), BF16),
        *[pltpu.VMEM((zs * 2, 1, W), F32)] * 2,
        pltpu.SemaphoreType.DMA((SEM.used,)),
    ]
    return pl.pallas_call(
        functools.partial(kernel, zs),
        out_shape=jax.ShapeDtypeStruct((T, W), BF16),
        in_specs=[hbm] * 17,
        out_specs=hbm,
        scratch_shapes=scratch,
        compiler_params=pltpu.CompilerParams(
            collective_id=0, has_side_effects=True, vmem_limit_bytes=60 * 1024 * 1024
        ),
        name="layer",
    )(
        forget_pre,
        values_in,
        floor_gap.reshape(1, W),
        query_pre,
        gate_pre,
        head_gain.reshape(1, W),
        route_ids.T,
        expert_gate.reshape(D, W),
        stream,
        norm_gain.reshape(1, W),
        route_weights.T,
        out_proj,
        expert_up.reshape(D, W),
        shared_gate,
        shared_up,
        shared_down,
        expert_down.reshape(D, W),
    )


def solution(mesh):
    zs = mesh.shape["sp"] // 2
    finer = Mesh(mesh.devices.reshape(zs, 2, 4, 4), ("z", "c", "y", "x"))
    sp, tp = ("z", "c"), ("y", "x")
    in_specs = (
        P(sp, tp),
        P(sp, tp),
        P(sp, tp),
        P(sp, tp),
        P(tp),
        P(),
        P(sp, tp),
        P(None, tp),
        P(tp),
        P(sp, None),
        P(sp, None),
        P(sp, None, tp),
        P(sp, None, tp),
        P(sp, None, tp),
        P(None, tp),
        P(None, tp),
        P(None, tp),
    )
    return jax.shard_map(
        functools.partial(layer, zs),
        mesh=finer,
        in_specs=in_specs,
        out_specs=P(sp, tp),
        check_vma=False,
    )
```
